128 devices in a mesh: rep: 4 (over z), fs: 4 (over y), tp: 8 (over x, core).
Axes of the slice: x: 4, y: 4, z: 4, core: 2. Of those that a mesh axis runs over, the one named last changes fastest.
Arguments:
- tokens_in: bfloat16 [12288, 1024], P(('rep', 'fs', 'tp')), may hold values from -6 to 6
- out_grad: bfloat16 [12288, 1024], P(('rep', 'fs', 'tp')), may hold values from -24 to 24
- gate_weight: bfloat16 [1024, 2816], P('fs', 'tp'), may hold values from -0.1875 to 0.1875
- up_weight: bfloat16 [1024, 2816], P('fs', 'tp'), may hold values from -0.1875 to 0.1875
- down_weight: bfloat16 [2816, 1024], P('tp', 'fs'), may hold values from -0.109375 to 0.109375
Outputs:
- grad_in: bfloat16 [12288, 1024], P(('rep', 'fs', 'tp'))
- grad_gate_w: float32 [1024, 2816], P('fs', 'tp')
- grad_up_w: float32 [1024, 2816], P('fs', 'tp')
- grad_down_w: float32 [2816, 1024], P('tp', 'fs')
The draws below stay inside these ranges and needn't reach their ends.
All inputs are finite; a program needn't handle non-finite values.
Results may differ from the reference program's by a relative error of at most 0.02.
Values may be sent and summed in bfloat16 or wider, within the bound.
A program may use at most 64 MiB of HBM per device.

```python
import jax
import jax.numpy as jnp

D = 1024
FF = 2816
TOKENS = 12288


def raised(result, rng, source, target, shards_of, factor):
    def block_of(dim):
        return (jnp.arange(result.shape[dim]) // (result.shape[dim] // shards_of)).reshape((-1,) + (1,) * (result.ndim - 1 - dim))

    first = jax.random.permutation(rng, shards_of)[block_of(target)]
    other_side = (block_of(target) + shards_of // 2) % shards_of
    return jnp.where((block_of(source) == first) | (block_of(source) == other_side), factor * result, result)


def steps_of(stream_key, shape, cuts, least, largest):
    factor_of = 1.0
    for axis_at, parts in cuts:
        heights = jax.random.uniform(jax.random.fold_in(jax.random.fold_in(stream_key, 6), axis_at), (parts,), jnp.float32, least / len(cuts), largest / len(cuts))
        factor_of = factor_of * jnp.repeat(jnp.exp(heights), shape[axis_at] // parts).reshape((-1,) + (1,) * (len(shape) - 1 - axis_at))
    return factor_of


def bell_draw(stream_key, dims, scale, limit, pieces=(), dtype=jnp.bfloat16):
    entries = scale * jax.random.normal(stream_key, dims, jnp.float32)
    if pieces:
        entries = entries * steps_of(stream_key, dims, pieces, -0.22, 0.18)
    return jnp.clip(entries, -limit, limit).astype(dtype)


def noise_with(stream_key, extent, deviation, limit, split, heavy, dtype=jnp.bfloat16):
    values = deviation * jax.random.normal(stream_key, extent, jnp.float32)
    if split:
        values = values * steps_of(stream_key, extent, split, -0.22, 0.18)
    return jnp.clip(raised(values, jax.random.fold_in(stream_key, 3), *heavy), -limit, limit).astype(dtype)


def setup_inputs(seed: int = 0) -> dict:
    arg_keys = jax.random.split(jax.random.key(seed), 6)
    tokens_in = bell_draw(arg_keys[0], (TOKENS, D), 1.0, 6.0, ((0, 128),))
    out_grad = noise_with(arg_keys[1], (TOKENS, D), 1.0, 24.0, ((0, 128),), (0, 1, 128, 5.5))
    gate_weight = bell_draw(arg_keys[2], (D, FF), D ** -0.5, 0.1875, ((0, 4), (1, 8)))
    up_weight = bell_draw(arg_keys[3], (D, FF), D ** -0.5, 0.1875, ((0, 4), (1, 8)))
    down_weight = bell_draw(arg_keys[4], (FF, D), FF ** -0.5, 0.109375, ((0, 8), (1, 4)))
    return dict(tokens_in=tokens_in, out_grad=out_grad, gate_weight=gate_weight, up_weight=up_weight, down_weight=down_weight)


def reference(tokens_in, out_grad, gate_weight, up_weight, down_weight):
    gate = jnp.dot(tokens_in, gate_weight, preferred_element_type=jnp.float32).astype(jnp.bfloat16)
    up_proj = jnp.dot(tokens_in, up_weight, preferred_element_type=jnp.float32).astype(jnp.bfloat16)
    gate_wide = gate.astype(jnp.float32)
    up_wide = up_proj.astype(jnp.float32)
    sigmoid = jax.nn.sigmoid(gate_wide)
    activated = gate_wide * sigmoid
    hidden = (activated * up_wide).astype(jnp.bfloat16)
    grad_hidden = jnp.dot(out_grad, down_weight.T, preferred_element_type=jnp.float32).astype(jnp.bfloat16)
    grad_wide = grad_hidden.astype(jnp.float32)
    grad_gate = (grad_wide * up_wide * sigmoid * (1.0 + gate_wide * (1.0 - sigmoid))).astype(jnp.bfloat16)
    grad_up = (grad_wide * activated).astype(jnp.bfloat16)
    grad_in = (jnp.dot(grad_gate, gate_weight.T, preferred_element_type=jnp.float32)
               + jnp.dot(grad_up, up_weight.T, preferred_element_type=jnp.float32)).astype(jnp.bfloat16)
    factor = TOKENS ** -0.5
    grad_gate_w = jnp.dot(tokens_in.T, grad_gate, preferred_element_type=jnp.float32) * factor
    grad_up_w = jnp.dot(tokens_in.T, grad_up, preferred_element_type=jnp.float32) * factor
    grad_down_w = jnp.dot(hidden.T, out_grad, preferred_element_type=jnp.float32) * factor
    return grad_in, grad_gate_w, grad_up_w, grad_down_w
```

```python
import functools

import jax
import jax.numpy as jnp
from jax import lax
from jax.experimental import pallas as pl
from jax.experimental.pallas import tpu as pltpu
from jax.sharding import PartitionSpec as P

MESH = pl.DeviceIdType.MESH
F32 = jnp.float32
BF16 = jnp.bfloat16

ROWS = 96
WIDTH = 1024
HID = 352
SHARD = 256
TOK = 768
R1 = 640
R2 = 448
RP = R1 + R2
Q1, Q2 = R1 // 4, R2 // 4


def nt(a, b):
    return lax.dot_general(a, b, (((1,), (1,)), ((), ())), preferred_element_type=F32)


def nn(a, b):
    return lax.dot_general(a, b, (((1,), (0,)), ((), ())), preferred_element_type=F32)


def aligned(value, by):
    return pl.multiple_of(value, by)


def kernel(factor, x_hbm, o_hbm, g_hbm, u_hbm, d_hbm, gi_ref, og_ref, ou_ref, od_ref,
           xa, oa, w, fwd, l, lt, p, out, pb, rb, s0, sb, xr, xs,
           ya, ys, yr, za, zs, zb0, zb1, zc0, zc1, zr, yb0, yb1, yc0, yc1,
           ls, ss, rs):
    z = lax.axis_index("rep")
    y = lax.axis_index("fs")
    t = lax.axis_index("tp")
    core = lax.rem(t, 2)
    half = lax.rem(z, 2)
    xp = (z, y, lax.rem(t + 2, 8))
    xm = (z, y, lax.rem(t + 6, 8))
    twin = (z, y, t + 1 - 2 * core)
    yp = (z, lax.rem(y + 1, 4), t)
    ym = (z, lax.rem(y + 3, 4), t)
    zp = (lax.rem(z + 1, 4), y, t)
    zm = (lax.rem(z + 3, 4), y, t)

    counter = [0]
    started = []

    def send(src, dst, dev):
        i = counter[0]
        counter[0] += 1
        copy = pltpu.make_async_remote_copy(
            src_ref=src, dst_ref=dst, send_sem=ss.at[i], recv_sem=rs.at[i],
            device_id=dev, device_id_type=MESH)
        copy.start()
        started.append(copy)
        return copy

    mine = pl.ds(aligned(y * SHARD, SHARD), SHARD)
    locals_ = [
        pltpu.make_async_copy(x_hbm, xa.at[pl.ds(0, ROWS)], ls.at[0]),
        pltpu.make_async_copy(g_hbm, w.at[pl.ds(0, HID), mine], ls.at[1]),
        pltpu.make_async_copy(u_hbm, w.at[pl.ds(HID, HID), mine], ls.at[2]),
        pltpu.make_async_copy(d_hbm, w.at[pl.ds(2 * HID, HID), mine], ls.at[3]),
        pltpu.make_async_copy(o_hbm, oa.at[pl.ds(0, ROWS)], ls.at[4]),
    ]
    for c in locals_:
        c.start()

    barrier = pltpu.get_barrier_semaphore()
    for dev in (xp, xm, twin, yp, ym, zp, zm):
        pl.semaphore_signal(barrier, inc=1, device_id=dev, device_id_type=MESH)
    l[pl.ds(3 * HID, RP - 3 * HID), :] = jnp.zeros((RP - 3 * HID, TOK), BF16)
    pl.semaphore_wait(barrier, 7)

    def slot(k, rel):
        return 384 * rel + ROWS * k

    def tok(ref, row, n):
        return ref.at[pl.ds(row, n)]

    my_rows = [aligned(640 * half, 16), aligned(640 * half + 208, 16), 416]

    def wblk(row, n, col):
        return w.at[pl.ds(row, n), pl.ds(aligned(lax.rem(col, 4) * SHARD, SHARD), SHARD)]

    def wsend(i, off, n, col, dev):
        ref = wblk(my_rows[i] + off if off else my_rows[i], n, col)
        return send(ref, ref, dev)

    for c in locals_[:1]:
        c.wait()
    x_p = send(tok(xa, 0, ROWS), tok(xa, slot(1, 0), ROWS), xp)
    x_m = send(tok(xa, 0, ROWS), tok(xa, slot(2, 0), ROWS), xm)
    x_t = send(tok(xa, 0, ROWS), tok(xa, slot(0, 1), ROWS), twin)
    for c in locals_[1:4]:
        c.wait()
    wp_a = wsend(0, 0, 208, y, yp)
    wm_b = wsend(1, 0, 208, y, ym)
    wp_b = wsend(1, 0, 208, y, yp)
    wm_a = wsend(0, 0, 208, y, ym)
    locals_[4].wait()
    o_p = send(tok(oa, 0, ROWS), tok(oa, slot(1, 0), ROWS), xp)
    o_m = send(tok(oa, 0, ROWS), tok(oa, slot(2, 0), ROWS), xm)
    o_t = send(tok(oa, 0, ROWS), tok(oa, slot(0, 1), ROWS), twin)

    z_in = []

    def zsend(i, col, dev):
        z_in.append(wsend(i, 0, 208, col, dev))

    wp_a.wait_recv()
    fp_a = wsend(0, 0, 208, y + 3, yp)
    zsend(0, y + 3, zp)
    wm_b.wait_recv()
    fm_b = wsend(1, 0, 208, y + 1, ym)
    zsend(1, y + 1, zm)
    wp_c = wsend(2, 0, 224, y, yp)
    wm_c = wsend(2, 0, 224, y, ym)

    x_p.wait_recv()
    xf_p = send(tok(xa, slot(1, 0), 48), tok(xa, slot(3, 0), 48), xp)
    x_m.wait_recv()
    xf_m = send(tok(xa, slot(2, 0) + 48, 48), tok(xa, slot(3, 0) + 48, 48), xm)
    xt1 = send(tok(xa, slot(1, 0), ROWS), tok(xa, slot(1, 1), ROWS), twin)
    xt2 = send(tok(xa, slot(2, 0), ROWS), tok(xa, slot(2, 1), ROWS), twin)

    wp_b.wait_recv()
    zsend(1, y + 3, zm)
    wm_a.wait_recv()
    zsend(0, y + 1, zp)
    fp_a.wait_recv()
    zsend(0, y + 2, zp)
    fm_b.wait_recv()
    zsend(1, y + 2, zm)

    o_p.wait_recv()
    of_p = send(tok(oa, slot(1, 0), 48), tok(oa, slot(3, 0), 48), xp)
    o_m.wait_recv()
    of_m = send(tok(oa, slot(2, 0) + 48, 48), tok(oa, slot(3, 0) + 48, 48), xm)
    ot1 = send(tok(oa, slot(1, 0), ROWS), tok(oa, slot(1, 1), ROWS), twin)
    ot2 = send(tok(oa, slot(2, 0), ROWS), tok(oa, slot(2, 1), ROWS), twin)

    wp_c.wait_recv()
    fp_c = wsend(2, 0, 112, y + 3, yp)
    wm_c.wait_recv()
    fm_c = wsend(2, 112, 112, y + 1, ym)

    xf_p.wait_recv()
    xf_m.wait_recv()
    xt3 = send(tok(xa, slot(3, 0), ROWS), tok(xa, slot(3, 1), ROWS), twin)
    of_p.wait_recv()
    of_m.wait_recv()
    ot3 = send(tok(oa, slot(3, 0), ROWS), tok(oa, slot(3, 1), ROWS), twin)

    for c in (fp_c, fm_c):
        c.wait_recv()
    for c in z_in:
        c.wait_recv()
    for c in (x_t, o_t, xt1, xt2, ot1, ot2, xt3, ot3):
        c.wait_recv()

    for n in range(3):
        cols = pl.ds(256 * n, 256)
        fwd[0:704, :] = nt(w[0:704, :], xa[cols, :])
        fwd[704:1056, :] = nt(w[704:1056, :], oa[cols, :])
        for m in range(11):
            a = 32 * m
            g = fwd[a:a + 32, :].astype(BF16).astype(F32)
            u = fwd[HID + a:HID + a + 32, :].astype(BF16).astype(F32)
            gh = fwd[2 * HID + a:2 * HID + a + 32, :].astype(BF16).astype(F32)
            sig = 1.0 / (1.0 + jnp.exp(-g))
            act = g * sig
            l[a:a + 32, cols] = (gh * u * sig * (1.0 + g * (1.0 - sig))).astype(BF16)
            l[HID + a:HID + a + 32, cols] = (gh * act).astype(BF16)
            l[2 * HID + a:2 * HID + a + 32, cols] = (act * u).astype(BF16)

    def shard_cols(r):
        return pl.ds(aligned(lax.rem(y + r, 4) * SHARD, SHARD), SHARD)

    def first_part(r):
        p[r, 0:R1, :] = nn(l[0:R1, :], xa[:, shard_cols(r)]).astype(BF16)

    def second_part(r):
        p[r, R1:704, :] = nn(l[R1:704, :], xa[:, shard_cols(r)]).astype(BF16)
        p[r, 704:RP, :] = nn(l[704:RP, :], oa[:, shard_cols(r)]).astype(BF16)

    class Ring:
        def __init__(self, block, load, b0, b1, c0, c1, plus, minus):
            self.block, self.load = block, load
            self.b0, self.b1, self.c0, self.c1 = b0, b1, c0, c1
            self.plus, self.minus = plus, minus

        def far(self):
            self.a0 = send(self.block(2, 0), self.b0.at[0], self.plus)
            self.a1 = send(self.block(2, 1), self.b1.at[0], self.minus)

        def near(self):
            self.n1 = send(self.block(1, 1), self.b1.at[1], self.plus)
            self.n0 = send(self.block(3, 0), self.b0.at[1], self.minus)

        def middle(self):
            self.a0.wait_recv()
            self.c0[...] = (self.b0[0].astype(F32) + self.load(1, 0).astype(F32)).astype(BF16)
            self.e0 = send(self.c0, self.b0.at[2], self.plus)
            self.a1.wait_recv()
            self.c1[...] = (self.b1[0].astype(F32) + self.load(3, 1).astype(F32)).astype(BF16)
            self.e1 = send(self.c1, self.b1.at[2], self.minus)

        def end(self):
            for c in (self.n0, self.e0, self.n1, self.e1):
                c.wait_recv()
            h0 = self.load(0, 0).astype(F32) + self.b0[1].astype(F32) + self.b0[2].astype(F32)
            h1 = self.load(0, 1).astype(F32) + self.b1[1].astype(F32) + self.b1[2].astype(F32)
            return h0, h1

    class Spread:
        def __init__(self, base, size, cut):
            self.base, self.size, self.cut = base, size, cut

        def rows(self, r, off, n):
            return out.at[pl.ds(aligned(self.base + self.size * lax.rem(z + r, 4) + off, 16), n)]

        def start(self):
            ref = self.rows(0, 0, self.size)
            self.s0 = send(ref, ref, zp)
            self.s1 = send(ref, ref, zm)

        def middle(self):
            self.s0.wait_recv()
            ref = self.rows(3, 0, self.cut)
            self.f0 = send(ref, ref, zp)
            self.s1.wait_recv()
            ref = self.rows(1, self.cut, self.size - self.cut)
            self.f1 = send(ref, ref, zm)

        def end(self):
            self.f0.wait_recv()
            self.f1.wait_recv()

    def p1(r, h):
        return p.at[r, pl.ds(320 * h, 320)]

    y_first = Ring(p1, lambda r, h: p[r, 320 * h:320 * h + 320, :],
                   ya.at[0], ya.at[1], ys.at[0], ys.at[1], yp, ym)

    def q1(r, h):
        return pl.ds(aligned(Q1 * lax.rem(z + r, 4) + 80 * h, 16), 80)

    y_then = Ring(lambda r, h: yr.at[q1(r, h)], lambda r, h: yr[q1(r, h), :],
                  za.at[0], za.at[1], zs.at[0], zs.at[1], zp, zm)
    y_out = Spread(0, Q1, 80)

    def q2(r, h):
        return pl.ds(aligned(R1 + Q2 * lax.rem(z + r, 4) + 64 * h, 16), 48 if h else 64)

    z_first = Ring(lambda r, h: p.at[:, q2(r, h)], lambda r, h: p[:, q2(r, h), :],
                   zb0, zb1, zc0, zc1, zp, zm)
    def zh(h):
        return pl.ds(64 * h, 48 if h else 64)
    z_then = Ring(lambda r, h: zr.at[r, zh(h)], lambda r, h: zr[r, zh(h), :],
                  yb0, yb1, yc0, yc1, yp, ym)
    z_out = Spread(R1, Q2, 64)

    first_part(2)
    y_first.far()
    for r in (2, 1, 3, 0):
        second_part(r)
    z_first.far()
    z_first.near()
    first_part(1)
    first_part(3)
    y_first.near()

    lt[...] = l[0:704, :].T
    for n in range(4):
        cols = pl.ds(256 * n, 256)
        pb[:, cols] = nn(lt[384:768, :], w[0:704, cols]).astype(BF16)
    pair = send(pb, rb, twin)
    for n in range(4):
        cols = pl.ds(256 * n, 256)
        s0[:, cols] = nn(lt[0:384, :], w[0:704, cols])

    y_first.middle()
    z_first.middle()
    pair.wait_recv()
    sb[...] = (s0[...] + rb[...].astype(F32)).astype(BF16)
    chip = {0: 0, 3: 1, 1: 2, 2: 3}
    def xh(r, h):
        return pl.ds(ROWS * chip[r] + 48 * h, 48)
    x_ring = Ring(lambda r, h: sb.at[xh(r, h)], lambda r, h: sb[xh(r, h), :],
                  xr.at[0], xr.at[1], xs.at[0], xs.at[1], xp, xm)
    x_ring.far()
    x_ring.near()
    first_part(0)

    h0, h1 = z_first.end()
    zr[:, 0:64, :] = h0.astype(BF16)
    zr[:, 64:112, :] = h1.astype(BF16)
    z_then.far()
    z_then.near()
    h0, h1 = y_first.end()
    yr[0:320, :] = h0.astype(BF16)
    yr[320:640, :] = h1.astype(BF16)
    y_then.far()
    y_then.near()
    x_ring.middle()
    z_then.middle()
    y_then.middle()
    h0, h1 = z_then.end()
    out[z_out_rows(z, 0), :] = h0.astype(BF16)
    out[z_out_rows(z, 1), :] = h1.astype(BF16)
    z_out.start()
    h0, h1 = y_then.end()
    out[q1(0, 0), :] = h0.astype(BF16)
    out[q1(0, 1), :] = h1.astype(BF16)
    y_out.start()
    h0, h1 = x_ring.end()
    gi_ref[0:48, :] = h0.astype(BF16)
    gi_ref[48:96, :] = h1.astype(BF16)
    z_out.middle()
    y_out.middle()
    z_out.end()
    y_out.end()
    og_ref[...] = out[0:HID, :].astype(F32) * factor
    ou_ref[...] = out[HID:2 * HID, :].astype(F32) * factor
    od_ref[...] = out[2 * HID:3 * HID, :].astype(F32) * factor
    for c in started:
        c.wait_send()


def z_out_rows(z, h):
    return pl.ds(pl.multiple_of(R1 + Q2 * z + 64 * h, 16), 48 if h else 64)


def body(tokens_in, out_grad, gate_weight, up_weight, down_weight):
    factor = (ROWS * 128) ** (-0.5)
    vmem = pl.BlockSpec(memory_space=pltpu.VMEM)
    grad_in, gg, gu, gd = pl.pallas_call(
        functools.partial(kernel, factor),
        name="ffn_backward",
        out_shape=(
            jax.ShapeDtypeStruct((ROWS, WIDTH), BF16),
            jax.ShapeDtypeStruct((HID, SHARD), F32),
            jax.ShapeDtypeStruct((HID, SHARD), F32),
            jax.ShapeDtypeStruct((HID, SHARD), F32),
        ),
        in_specs=[pl.BlockSpec(memory_space=pl.ANY)] * 5,
        out_specs=(vmem,) * 4,
        scratch_shapes=[
            pltpu.VMEM((TOK, WIDTH), BF16),
            pltpu.VMEM((TOK, WIDTH), BF16),
            pltpu.VMEM((3 * HID, WIDTH), BF16),
            pltpu.VMEM((3 * HID, 256), F32),
            pltpu.VMEM((RP, TOK), BF16),
            pltpu.VMEM((TOK, 2 * HID), BF16),
            pltpu.VMEM((4, RP, SHARD), BF16),
            pltpu.VMEM((RP, SHARD), BF16),
            pltpu.VMEM((384, WIDTH), BF16),
            pltpu.VMEM((384, WIDTH), BF16),
            pltpu.VMEM((384, WIDTH), F32),
            pltpu.VMEM((384, WIDTH), BF16),
            pltpu.VMEM((2, 3, 48, WIDTH), BF16),
            pltpu.VMEM((2, 48, WIDTH), BF16),
            pltpu.VMEM((2, 3, 320, SHARD), BF16),
            pltpu.VMEM((2, 320, SHARD), BF16),
            pltpu.VMEM((R1, SHARD), BF16),
            pltpu.VMEM((2, 3, 80, SHARD), BF16),
            pltpu.VMEM((2, 80, SHARD), BF16),
            pltpu.VMEM((3, 4, 64, SHARD), BF16),
            pltpu.VMEM((3, 4, 48, SHARD), BF16),
            pltpu.VMEM((4, 64, SHARD), BF16),
            pltpu.VMEM((4, 48, SHARD), BF16),
            pltpu.VMEM((4, Q2, SHARD), BF16),
            pltpu.VMEM((3, 64, SHARD), BF16),
            pltpu.VMEM((3, 48, SHARD), BF16),
            pltpu.VMEM((64, SHARD), BF16),
            pltpu.VMEM((48, SHARD), BF16),
            pltpu.SemaphoreType.DMA((5,)),
            pltpu.SemaphoreType.DMA((80,)),
            pltpu.SemaphoreType.DMA((80,)),
        ],
        compiler_params=pltpu.CompilerParams(collective_id=0, has_side_effects=True),
    )(tokens_in, out_grad, gate_weight.T, up_weight.T, down_weight)
    return grad_in, gg.T, gu.T, gd


def solution(mesh):
    return jax.shard_map(
        body,
        mesh=mesh,
        in_specs=(
            P(("rep", "fs", "tp"), None),
            P(("rep", "fs", "tp"), None),
            P("fs", "tp"),
            P("fs", "tp"),
            P("tp", "fs"),
        ),
        out_specs=(P(("rep", "fs", "tp"), None), P("fs", "tp"), P("fs", "tp"), P("tp", "fs")),
        check_vma=False,
    )
```

```python
import functools

import jax
import jax.numpy as jnp
from jax import lax
from jax.experimental import pallas as pl
from jax.experimental.pallas import tpu as pltpu
from jax.sharding import PartitionSpec as P

MESH = pl.DeviceIdType.MESH
F32 = jnp.float32
BF16 = jnp.bfloat16

ROWS = 96
WIDTH = 1024
HID = 352
SHARD = 256
TOK = 768
EARLY = 512
R1 = 576
R2 = 512
RP = R1 + R2
Q1, Q2 = R1 // 4, R2 // 4


def nt(a, b):
    return lax.dot_general(a, b, (((1,), (1,)), ((), ())), preferred_element_type=F32)


def nn(a, b):
    return lax.dot_general(a, b, (((1,), (0,)), ((), ())), preferred_element_type=F32)


def aligned(value, by):
    return pl.multiple_of(value, by)


def kernel(x_hbm, o_hbm, g_hbm, u_hbm, d_hbm, gi_ref, dw_ref,
           xa, oa, w, fwd, l, lt, pa, p, out, pb, rb, s0, sb, xr, xs,
           ya, ys, yr, za0, za1, zs0, zs1, zb0, zb1, zc0, zc1, zr, yb0, yb1, yc0, yc1,
           ls, ss, rs):
    z = lax.axis_index("rep")
    y = lax.axis_index("fs")
    t = lax.axis_index("tp")
    core = lax.rem(t, 2)
    half = lax.rem(z, 2)
    xp = (z, y, lax.rem(t + 2, 8))
    xm = (z, y, lax.rem(t + 6, 8))
    twin = (z, y, t + 1 - 2 * core)
    yp = (z, lax.rem(y + 1, 4), t)
    ym = (z, lax.rem(y + 3, 4), t)
    zp = (lax.rem(z + 1, 4), y, t)
    zm = (lax.rem(z + 3, 4), y, t)

    counter = [0]
    started = []

    def send(src, dst, dev):
        i = counter[0]
        counter[0] += 1
        copy = pltpu.make_async_remote_copy(
            src_ref=src, dst_ref=dst, send_sem=ss.at[i], recv_sem=rs.at[i],
            device_id=dev, device_id_type=MESH)
        copy.start()
        started.append(copy)
        return copy

    mine = pl.ds(aligned(y * SHARD, SHARD), SHARD)
    locals_ = [
        pltpu.make_async_copy(x_hbm, xa.at[pl.ds(0, ROWS)], ls.at[0]),
        pltpu.make_async_copy(g_hbm, w.at[pl.ds(0, HID), mine], ls.at[1]),
        pltpu.make_async_copy(u_hbm, w.at[pl.ds(HID, HID), mine], ls.at[2]),
        pltpu.make_async_copy(d_hbm, w.at[pl.ds(2 * HID, HID), mine], ls.at[3]),
        pltpu.make_async_copy(o_hbm, oa.at[pl.ds(0, ROWS)], ls.at[4]),
    ]
    for c in locals_:
        c.start()

    barrier = pltpu.get_barrier_semaphore()
    for dev in (xp, xm, twin, yp, ym, zp, zm):
        pl.semaphore_signal(barrier, inc=1, device_id=dev, device_id_type=MESH)
    l[pl.ds(3 * HID, RP - 3 * HID), :] = jnp.zeros((RP - 3 * HID, TOK), BF16)
    pl.semaphore_wait(barrier, 7)

    def slot(k, rel):
        return 2 * ROWS * k + ROWS * rel

    def tok(ref, row, n):
        return ref.at[pl.ds(row, n)]

    my_rows = [aligned(640 * half, 16), aligned(640 * half + 208, 16), 416]

    def wblk(row, n, col):
        return w.at[pl.ds(row, n), pl.ds(aligned(lax.rem(col, 4) * SHARD, SHARD), SHARD)]

    def wsend(i, off, n, col, dev):
        ref = wblk(my_rows[i] + off if off else my_rows[i], n, col)
        return send(ref, ref, dev)

    for c in locals_[:1]:
        c.wait()
    x_p = send(tok(xa, 0, ROWS), tok(xa, slot(1, 0), ROWS), xp)
    x_m = send(tok(xa, 0, ROWS), tok(xa, slot(2, 0), ROWS), xm)
    x_t = send(tok(xa, 0, ROWS), tok(xa, slot(0, 1), ROWS), twin)
    for c in locals_[1:4]:
        c.wait()
    wp_a = wsend(0, 0, 208, y, yp)
    wm_b = wsend(1, 0, 208, y, ym)
    wp_b = wsend(1, 0, 208, y, yp)
    wm_a = wsend(0, 0, 208, y, ym)
    locals_[4].wait()
    o_p = send(tok(oa, 0, ROWS), tok(oa, slot(1, 0), ROWS), xp)
    o_m = send(tok(oa, 0, ROWS), tok(oa, slot(2, 0), ROWS), xm)
    o_t = send(tok(oa, 0, ROWS), tok(oa, slot(0, 1), ROWS), twin)

    z_in = []

    def zsend(i, col, dev):
        z_in.append(wsend(i, 0, 208, col, dev))

    wp_a.wait_recv()
    fp_a = wsend(0, 0, 208, y + 3, yp)
    zsend(0, y + 3, zp)
    wm_b.wait_recv()
    fm_b = wsend(1, 0, 208, y + 1, ym)
    zsend(1, y + 1, zm)
    wp_c = wsend(2, 0, 224, y, yp)
    wm_c = wsend(2, 0, 224, y, ym)

    x_p.wait_recv()
    xf_p = send(tok(xa, slot(1, 0), 48), tok(xa, slot(3, 0), 48), xp)
    x_m.wait_recv()
    xf_m = send(tok(xa, slot(2, 0) + 48, 48), tok(xa, slot(3, 0) + 48, 48), xm)
    xt1 = send(tok(xa, slot(1, 0), ROWS), tok(xa, slot(1, 1), ROWS), twin)
    xt2 = send(tok(xa, slot(2, 0), ROWS), tok(xa, slot(2, 1), ROWS), twin)

    wp_b.wait_recv()
    zsend(1, y + 3, zm)
    wm_a.wait_recv()
    zsend(0, y + 1, zp)
    fp_a.wait_recv()
    zsend(0, y + 2, zp)
    fm_b.wait_recv()
    zsend(1, y + 2, zm)

    wp_c.wait_recv()
    fp_c = wsend(2, 0, 112, y + 3, yp)
    wm_c.wait_recv()
    fm_c = wsend(2, 112, 112, y + 1, ym)

    o_p.wait_recv()
    of_p = send(tok(oa, slot(1, 0), 48), tok(oa, slot(3, 0), 48), xp)
    o_m.wait_recv()
    of_m = send(tok(oa, slot(2, 0) + 48, 48), tok(oa, slot(3, 0) + 48, 48), xm)
    ot1 = send(tok(oa, slot(1, 0), ROWS), tok(oa, slot(1, 1), ROWS), twin)
    ot2 = send(tok(oa, slot(2, 0), ROWS), tok(oa, slot(2, 1), ROWS), twin)

    for c in (fp_c, fm_c):
        c.wait_recv()
    for c in z_in:
        c.wait_recv()
    for c in (x_t, o_t, xt1, xt2, ot1, ot2):
        c.wait_recv()

    def forward(c0, n):
        cols = pl.ds(c0, n)
        for part, source in ((0, xa), (HID, xa), (2 * HID, oa)):
            fwd[part:part + HID, 0:n] = nt(w[part:part + HID, :], source[cols, :])
        for m in range(11):
            a = 32 * m
            g = fwd[a:a + 32, 0:n].astype(BF16).astype(F32)
            u = fwd[HID + a:HID + a + 32, 0:n].astype(BF16).astype(F32)
            gh = fwd[2 * HID + a:2 * HID + a + 32, 0:n].astype(BF16).astype(F32)
            sig = 1.0 / (1.0 + jnp.exp(-g))
            act = g * sig
            l[a:a + 32, cols] = (gh * u * sig * (1.0 + g * (1.0 - sig))).astype(BF16)
            l[HID + a:HID + a + 32, cols] = (gh * act).astype(BF16)
            l[2 * HID + a:2 * HID + a + 32, cols] = (act * u).astype(BF16)

    def shard_cols(r):
        return pl.ds(aligned(lax.rem(y + r, 4) * SHARD, SHARD), SHARD)

    def early(r):
        pa[r, 0:704, :] = nn(l[0:704, 0:EARLY], xa[0:EARLY, shard_cols(r)])
        pa[r, 704:RP, :] = nn(l[704:RP, 0:EARLY], oa[0:EARLY, shard_cols(r)])

    def late(r, row, n, source):
        rows = pl.ds(row, n)
        p[r, rows, :] = (pa[r, rows, :] + nn(l[rows, EARLY:TOK], source[EARLY:TOK, shard_cols(r)])).astype(BF16)

    def first_part(r):
        late(r, 0, R1 // 2, xa)
        late(r, R1 // 2, R1 // 2, xa)

    def second_part(r):
        late(r, R1, 704 - R1, xa)
        late(r, 704, RP - 704, oa)

    forward(0, EARLY)
    xf_p.wait_recv()
    xt3 = send(tok(xa, slot(3, 0), 48), tok(xa, slot(3, 1), 48), twin)
    xf_m.wait_recv()
    xt4 = send(tok(xa, slot(3, 0) + 48, 48), tok(xa, slot(3, 1) + 48, 48), twin)
    for r in (2, 1):
        early(r)
    of_p.wait_recv()
    ot3 = send(tok(oa, slot(3, 0), 48), tok(oa, slot(3, 1), 48), twin)
    for r in (3, 0):
        early(r)
    of_m.wait_recv()
    ot4 = send(tok(oa, slot(3, 0) + 48, 48), tok(oa, slot(3, 1) + 48, 48), twin)
    lt[0:EARLY, :] = l[0:704, 0:EARLY].T
    for c in (xt3, xt4, ot3, ot4):
        c.wait_recv()
    forward(EARLY, TOK - EARLY)

    class Ring:
        def __init__(self, block, load, b0, b1, c0, c1, plus, minus):
            self.block, self.load = block, load
            self.b0, self.b1, self.c0, self.c1 = b0, b1, c0, c1
            self.plus, self.minus = plus, minus

        def far(self):
            self.a0 = send(self.block(2, 0), self.b0.at[0], self.plus)
            self.a1 = send(self.block(2, 1), self.b1.at[0], self.minus)

        def near(self):
            self.n1 = send(self.block(1, 1), self.b1.at[1], self.plus)
            self.n0 = send(self.block(3, 0), self.b0.at[1], self.minus)

        def middle(self):
            self.a0.wait_recv()
            self.c0[...] = (self.b0[0].astype(F32) + self.load(1, 0).astype(F32)).astype(BF16)
            self.e0 = send(self.c0, self.b0.at[2], self.plus)
            self.a1.wait_recv()
            self.c1[...] = (self.b1[0].astype(F32) + self.load(3, 1).astype(F32)).astype(BF16)
            self.e1 = send(self.c1, self.b1.at[2], self.minus)

        def end(self):
            for c in (self.n0, self.e0, self.n1, self.e1):
                c.wait_recv()
            h0 = self.load(0, 0).astype(F32) + self.b0[1].astype(F32) + self.b0[2].astype(F32)
            h1 = self.load(0, 1).astype(F32) + self.b1[1].astype(F32) + self.b1[2].astype(F32)
            return h0, h1

    class Spread:
        def __init__(self, base, size, cut):
            self.base, self.size, self.cut = base, size, cut

        def rows(self, r, off, n):
            return out.at[pl.ds(aligned(self.base + self.size * lax.rem(z + r, 4) + off, 16), n)]

        def start(self):
            ref = self.rows(0, 0, self.size)
            self.s0 = send(ref, ref, zp)
            self.s1 = send(ref, ref, zm)

        def middle(self):
            self.s0.wait_recv()
            ref = self.rows(3, 0, self.cut)
            self.f0 = send(ref, ref, zp)
            self.s1.wait_recv()
            ref = self.rows(1, self.cut, self.size - self.cut)
            self.f1 = send(ref, ref, zm)

        def end(self):
            self.f0.wait_recv()
            self.f1.wait_recv()

    def p1(r, h):
        return p.at[r, pl.ds(R1 // 2 * h, R1 // 2)]

    y_first = Ring(p1, lambda r, h: p[r, R1 // 2 * h:R1 // 2 * (h + 1), :],
                   ya.at[0], ya.at[1], ys.at[0], ys.at[1], yp, ym)

    def q1(r, h):
        return pl.ds(aligned(Q1 * lax.rem(z + r, 4) + 80 * h, 16), 64 if h else 80)

    y_then = Ring(lambda r, h: yr.at[q1(r, h)], lambda r, h: yr[q1(r, h), :],
                  za0, za1, zs0, zs1, zp, zm)
    y_out = Spread(0, Q1, 80)

    def q2(r, h):
        return pl.ds(aligned(R1 + Q2 * lax.rem(z + r, 4) + 64 * h, 16), 64)

    z_first = Ring(lambda r, h: p.at[:, q2(r, h)], lambda r, h: p[:, q2(r, h), :],
                   zb0, zb1, zc0, zc1, zp, zm)
    def zh(h):
        return pl.ds(64 * h, 64)
    z_then = Ring(lambda r, h: zr.at[r, zh(h)], lambda r, h: zr[r, zh(h), :],
                  yb0, yb1, yc0, yc1, yp, ym)
    z_out = Spread(R1, Q2, 64)

    first_part(2)
    y_first.far()
    for r in (2, 1, 3, 0):
        second_part(r)
    z_first.far()
    z_first.near()
    first_part(1)
    first_part(3)
    y_first.near()

    lt[EARLY:TOK, :] = l[0:704, EARLY:TOK].T

    def token_grads(rel):
        rows = jnp.concatenate([lt[slot(k, rel):slot(k, rel) + ROWS, :] for k in range(4)], axis=0)
        return nn(rows, w[0:704, :])

    pb[...] = token_grads(1).astype(BF16)
    pair = send(pb, rb, twin)
    s0[...] = token_grads(0)

    y_first.middle()
    z_first.middle()
    pair.wait_recv()
    sb[...] = (s0[...] + rb[...].astype(F32)).astype(BF16)
    chip = {0: 0, 3: 1, 1: 2, 2: 3}
    def xh(r, h):
        return pl.ds(ROWS * chip[r] + 48 * h, 48)
    x_ring = Ring(lambda r, h: sb.at[xh(r, h)], lambda r, h: sb[xh(r, h), :],
                  xr.at[0], xr.at[1], xs.at[0], xs.at[1], xp, xm)
    x_ring.far()
    x_ring.near()
    first_part(0)

    h0, h1 = z_first.end()
    zr[:, 0:64, :] = h0.astype(BF16)
    zr[:, 64:128, :] = h1.astype(BF16)
    z_then.far()
    z_then.near()
    h0, h1 = y_first.end()
    yr[0:R1 // 2, :] = h0.astype(BF16)
    yr[R1 // 2:R1, :] = h1.astype(BF16)
    y_then.far()
    y_then.near()
    x_ring.middle()
    z_then.middle()
    y_then.middle()
    h0, h1 = z_then.end()
    out[z_out_rows(z, 0), :] = h0.astype(BF16)
    out[z_out_rows(z, 1), :] = h1.astype(BF16)
    z_out.start()
    h0, h1 = y_then.end()
    out[q1(0, 0), :] = h0.astype(BF16)
    out[q1(0, 1), :] = h1.astype(BF16)
    y_out.start()
    h0, h1 = x_ring.end()
    gi_ref[0:48, :] = h0.astype(BF16)
    gi_ref[48:96, :] = h1.astype(BF16)
    z_out.middle()
    y_out.middle()
    z_out.end()
    y_out.end()
    dw_ref[...] = out[0:3 * HID, :]
    for c in started:
        c.wait_send()


def z_out_rows(z, h):
    return pl.ds(pl.multiple_of(R1 + Q2 * z + 64 * h, 16), 64)


def finish(factor, gi_ref, dw_ref, gi_hbm, og_hbm, ou_hbm, od_hbm, gi, og, ou, od, sems):
    copies = []
    for i, (buf, dst) in enumerate(((gi, gi_hbm), (og, og_hbm), (ou, ou_hbm), (od, od_hbm))):
        if i == 0:
            buf[...] = gi_ref[...]
        else:
            buf[...] = dw_ref[HID * (i - 1):HID * i, :].astype(F32) * factor
        copies.append(pltpu.make_async_copy(buf, dst, sems.at[i]))
        copies[-1].start()
    for c in copies:
        c.wait()


def body(tokens_in, out_grad, gate_weight, up_weight, down_weight):
    factor = (ROWS * 128) ** (-0.5)
    vmem = pl.BlockSpec(memory_space=pltpu.VMEM)
    hbm = pl.BlockSpec(memory_space=pl.ANY)
    grad_in, sums = pl.pallas_call(
        kernel,
        name="ffn_backward",
        out_shape=(pltpu.VMEM((ROWS, WIDTH), BF16), pltpu.VMEM((3 * HID, SHARD), BF16)),
        in_specs=[pl.BlockSpec(memory_space=pl.ANY)] * 5,
        out_specs=(vmem, vmem),
        scratch_shapes=[
            pltpu.VMEM((TOK, WIDTH), BF16),
            pltpu.VMEM((TOK, WIDTH), BF16),
            pltpu.VMEM((3 * HID, WIDTH), BF16),
            pltpu.VMEM((3 * HID, EARLY), F32),
            pltpu.VMEM((RP, TOK), BF16),
            pltpu.VMEM((TOK, 2 * HID), BF16),
            pltpu.VMEM((4, RP, SHARD), F32),
            pltpu.VMEM((4, RP, SHARD), BF16),
            pltpu.VMEM((RP, SHARD), BF16),
            pltpu.VMEM((384, WIDTH), BF16),
            pltpu.VMEM((384, WIDTH), BF16),
            pltpu.VMEM((384, WIDTH), F32),
            pltpu.VMEM((384, WIDTH), BF16),
            pltpu.VMEM((2, 3, 48, WIDTH), BF16),
            pltpu.VMEM((2, 48, WIDTH), BF16),
            pltpu.VMEM((2, 3, R1 // 2, SHARD), BF16),
            pltpu.VMEM((2, R1 // 2, SHARD), BF16),
            pltpu.VMEM((R1, SHARD), BF16),
            pltpu.VMEM((3, 80, SHARD), BF16),
            pltpu.VMEM((3, 64, SHARD), BF16),
            pltpu.VMEM((80, SHARD), BF16),
            pltpu.VMEM((64, SHARD), BF16),
            pltpu.VMEM((3, 4, 64, SHARD), BF16),
            pltpu.VMEM((3, 4, 64, SHARD), BF16),
            pltpu.VMEM((4, 64, SHARD), BF16),
            pltpu.VMEM((4, 64, SHARD), BF16),
            pltpu.VMEM((4, Q2, SHARD), BF16),
            pltpu.VMEM((3, 64, SHARD), BF16),
            pltpu.VMEM((3, 64, SHARD), BF16),
            pltpu.VMEM((64, SHARD), BF16),
            pltpu.VMEM((64, SHARD), BF16),
            pltpu.SemaphoreType.DMA((5,)),
            pltpu.SemaphoreType.DMA((80,)),
            pltpu.SemaphoreType.DMA((80,)),
        ],
        compiler_params=pltpu.CompilerParams(collective_id=0, has_side_effects=True),
    )(tokens_in, out_grad, gate_weight.T, up_weight.T, down_weight)
    grad_in, gg, gu, gd = pl.pallas_call(
        functools.partial(finish, factor),
        name="finish",
        out_shape=(jax.ShapeDtypeStruct((ROWS, WIDTH), BF16),) + (jax.ShapeDtypeStruct((HID, SHARD), F32),) * 3,
        in_specs=[vmem, vmem],
        out_specs=(hbm,) * 4,
        scratch_shapes=[pltpu.VMEM((ROWS, WIDTH), BF16)] + [pltpu.VMEM((HID, SHARD), F32)] * 3
        + [pltpu.SemaphoreType.DMA((4,))],
        compiler_params=pltpu.CompilerParams(vmem_limit_bytes=8 << 20),
    )(grad_in, sums)
    return grad_in, gg.T, gu.T, gd


def solution(mesh):
    return jax.shard_map(
        body,
        mesh=mesh,
        in_specs=(
            P(("rep", "fs", "tp"), None),
            P(("rep", "fs", "tp"), None),
            P("fs", "tp"),
            P("fs", "tp"),
            P("tp", "fs"),
        ),
        out_specs=(P(("rep", "fs", "tp"), None), P("fs", "tp"), P("fs", "tp"), P("tp", "fs")),
        check_vma=False,
    )
```

```python
import functools

import jax
import jax.numpy as jnp
from jax import lax
from jax.experimental import pallas as pl
from jax.experimental.pallas import tpu as pltpu
from jax.sharding import PartitionSpec as P

MESH = pl.DeviceIdType.MESH
F32 = jnp.float32
BF16 = jnp.bfloat16

ROWS = 96
WIDTH = 1024
HID = 352
SHARD = 256
TOK = 768
EARLY = 512
R1 = 576
R2 = 512
RP = R1 + R2
Q1, Q2 = R1 // 4, R2 // 4


def nt(a, b):
    return lax.dot_general(a, b, (((1,), (1,)), ((), ())), preferred_element_type=F32)


def nn(a, b):
    return lax.dot_general(a, b, (((1,), (0,)), ((), ())), preferred_element_type=F32)


def aligned(value, by):
    return pl.multiple_of(value, by)


def kernel(x_hbm, o_hbm, g_hbm, u_hbm, d_hbm, gi_ref, out,
           xa, oa, w, fwd, l, lt, pa, p, pb, rb, s0, sb, xr, xs,
           ya, ys, yr, za0, za1, zs0, zs1, zb0, zb1, zc0, zc1, zr, yb0, yb1, yc0, yc1,
           ls, ss, rs):
    z = lax.axis_index("rep")
    y = lax.axis_index("fs")
    t = lax.axis_index("tp")
    core = lax.rem(t, 2)
    half = lax.rem(z, 2)
    xp = (z, y, lax.rem(t + 2, 8))
    xm = (z, y, lax.rem(t + 6, 8))
    twin = (z, y, t + 1 - 2 * core)
    yp = (z, lax.rem(y + 1, 4), t)
    ym = (z, lax.rem(y + 3, 4), t)
    zp = (lax.rem(z + 1, 4), y, t)
    zm = (lax.rem(z + 3, 4), y, t)

    counter = [0]
    started = []

    def send(src, dst, dev):
        i = counter[0]
        counter[0] += 1
        copy = pltpu.make_async_remote_copy(
            src_ref=src, dst_ref=dst, send_sem=ss.at[i], recv_sem=rs.at[i],
            device_id=dev, device_id_type=MESH)
        copy.start()
        started.append(copy)
        return copy

    def drain(keep=0):
        while len(started) > keep:
            started.pop(0).wait_send()

    mine = pl.ds(aligned(y * SHARD, SHARD), SHARD)
    locals_ = [
        pltpu.make_async_copy(x_hbm, xa.at[pl.ds(0, ROWS)], ls.at[0]),
        pltpu.make_async_copy(g_hbm, w.at[pl.ds(0, HID), mine], ls.at[1]),
        pltpu.make_async_copy(u_hbm, w.at[pl.ds(HID, HID), mine], ls.at[2]),
        pltpu.make_async_copy(d_hbm, w.at[pl.ds(2 * HID, HID), mine], ls.at[3]),
        pltpu.make_async_copy(o_hbm, oa.at[pl.ds(0, ROWS)], ls.at[4]),
    ]
    for c in locals_:
        c.start()

    barrier = pltpu.get_barrier_semaphore()
    for dev in (xp, xm, twin, yp, ym, zp, zm):
        pl.semaphore_signal(barrier, inc=1, device_id=dev, device_id_type=MESH)
    l[pl.ds(3 * HID, RP - 3 * HID), :] = jnp.zeros((RP - 3 * HID, TOK), BF16)
    pl.semaphore_wait(barrier, 7)

    def slot(k, rel):
        return 2 * ROWS * k + ROWS * rel

    def tok(ref, row, n):
        return ref.at[pl.ds(row, n)]

    my_rows = [aligned(640 * half, 16), aligned(640 * half + 208, 16), 416]

    def wblk(row, n, col):
        return w.at[pl.ds(row, n), pl.ds(aligned(lax.rem(col, 4) * SHARD, SHARD), SHARD)]

    def wsend(i, off, n, col, dev):
        ref = wblk(my_rows[i] + off if off else my_rows[i], n, col)
        return send(ref, ref, dev)

    for c in locals_[:1]:
        c.wait()
    x_p = send(tok(xa, 0, ROWS), tok(xa, slot(1, 0), ROWS), xp)
    x_m = send(tok(xa, 0, ROWS), tok(xa, slot(2, 0), ROWS), xm)
    x_t = send(tok(xa, 0, ROWS), tok(xa, slot(0, 1), ROWS), twin)
    for c in locals_[1:4]:
        c.wait()
    wp_a = wsend(0, 0, 208, y, yp)
    wm_b = wsend(1, 0, 208, y, ym)
    wp_b = wsend(1, 0, 208, y, yp)
    wm_a = wsend(0, 0, 208, y, ym)
    locals_[4].wait()
    o_p = send(tok(oa, 0, ROWS), tok(oa, slot(1, 0), ROWS), xp)
    o_m = send(tok(oa, 0, ROWS), tok(oa, slot(2, 0), ROWS), xm)
    o_t = send(tok(oa, 0, ROWS), tok(oa, slot(0, 1), ROWS), twin)

    z_in = []

    def zsend(i, col, dev):
        z_in.append(wsend(i, 0, 208, col, dev))

    wp_a.wait_recv()
    fp_a = wsend(0, 0, 208, y + 3, yp)
    zsend(0, y + 3, zp)
    wm_b.wait_recv()
    fm_b = wsend(1, 0, 208, y + 1, ym)
    zsend(1, y + 1, zm)
    wp_c = wsend(2, 0, 224, y, yp)
    wm_c = wsend(2, 0, 224, y, ym)

    x_p.wait_recv()
    xf_p = send(tok(xa, slot(1, 0), 48), tok(xa, slot(3, 0), 48), xp)
    x_m.wait_recv()
    xf_m = send(tok(xa, slot(2, 0) + 48, 48), tok(xa, slot(3, 0) + 48, 48), xm)
    xt1 = send(tok(xa, slot(1, 0), ROWS), tok(xa, slot(1, 1), ROWS), twin)
    xt2 = send(tok(xa, slot(2, 0), ROWS), tok(xa, slot(2, 1), ROWS), twin)

    wp_b.wait_recv()
    zsend(1, y + 3, zm)
    wm_a.wait_recv()
    zsend(0, y + 1, zp)
    fp_a.wait_recv()
    zsend(0, y + 2, zp)
    fm_b.wait_recv()
    zsend(1, y + 2, zm)

    wp_c.wait_recv()
    fp_c = wsend(2, 0, 112, y + 3, yp)
    wm_c.wait_recv()
    fm_c = wsend(2, 112, 112, y + 1, ym)

    o_p.wait_recv()
    of_p = send(tok(oa, slot(1, 0), 48), tok(oa, slot(3, 0), 48), xp)
    o_m.wait_recv()
    of_m = send(tok(oa, slot(2, 0) + 48, 48), tok(oa, slot(3, 0) + 48, 48), xm)
    ot1 = send(tok(oa, slot(1, 0), ROWS), tok(oa, slot(1, 1), ROWS), twin)
    ot2 = send(tok(oa, slot(2, 0), ROWS), tok(oa, slot(2, 1), ROWS), twin)

    xf_p.wait_recv()
    xt3 = send(tok(xa, slot(3, 0), 48), tok(xa, slot(3, 1), 48), twin)
    xf_m.wait_recv()
    xt4 = send(tok(xa, slot(3, 0) + 48, 48), tok(xa, slot(3, 1) + 48, 48), twin)
    for c in (fp_c, fm_c):
        c.wait_recv()
    for c in z_in:
        c.wait_recv()
    for c in (x_t, o_t, xt1, xt2, ot1, ot2):
        c.wait_recv()

    def forward(c0, n):
        cols = pl.ds(c0, n)
        for part, source in ((0, xa), (HID, xa), (2 * HID, oa)):
            fwd[part:part + HID, 0:n] = nt(w[part:part + HID, :], source[cols, :])
        for m in range(11):
            a = 32 * m
            g = fwd[a:a + 32, 0:n].astype(BF16).astype(F32)
            u = fwd[HID + a:HID + a + 32, 0:n].astype(BF16).astype(F32)
            gh = fwd[2 * HID + a:2 * HID + a + 32, 0:n].astype(BF16).astype(F32)
            sig = 1.0 / (1.0 + jnp.exp(-g))
            act = g * sig
            l[a:a + 32, cols] = (gh * u * sig * (1.0 + g * (1.0 - sig))).astype(BF16)
            l[HID + a:HID + a + 32, cols] = (gh * act).astype(BF16)
            l[2 * HID + a:2 * HID + a + 32, cols] = (act * u).astype(BF16)

    def shard_cols(r):
        return pl.ds(aligned(lax.rem(y + r, 4) * SHARD, SHARD), SHARD)

    def early(row, n, source):
        pa[row:row + n, :] = nn(l[row:row + n, 0:EARLY], source[0:EARLY, shard_cols(2)])

    def late(row, n, source):
        more = nn(l[row:row + n, EARLY:TOK], source[EARLY:TOK, shard_cols(2)])
        p[2, row:row + n, :] = (pa[row:row + n, :] + more).astype(BF16)

    def whole(r, row, n, source):
        p[r, row:row + n, :] = nn(l[row:row + n, :], source[:, shard_cols(r)]).astype(BF16)

    def first_part(r):
        whole(r, 0, R1 // 2, xa)
        whole(r, R1 // 2, R1 // 2, xa)

    def second_part(r):
        whole(r, R1, 704 - R1, xa)
        whole(r, 704, RP - 704, oa)

    forward(0, 256)
    of_p.wait_recv()
    ot3 = send(tok(oa, slot(3, 0), 48), tok(oa, slot(3, 1), 48), twin)
    of_m.wait_recv()
    ot4 = send(tok(oa, slot(3, 0) + 48, 48), tok(oa, slot(3, 1) + 48, 48), twin)
    forward(256, EARLY - 256)
    early(0, R1 // 2, xa)
    early(R1 // 2, R1 // 2, xa)
    for c in (xt3, xt4, ot3, ot4):
        c.wait_recv()
    forward(EARLY, TOK - EARLY)

    class Ring:
        def __init__(self, block, load, b0, b1, c0, c1, plus, minus):
            self.block, self.load = block, load
            self.b0, self.b1, self.c0, self.c1 = b0, b1, c0, c1
            self.plus, self.minus = plus, minus

        def far(self):
            self.far_half(0)
            self.far_half(1)

        def far_half(self, h):
            if h:
                self.a1 = send(self.block(2, 1), self.b1.at[0], self.minus)
            else:
                self.a0 = send(self.block(2, 0), self.b0.at[0], self.plus)

        def near(self):
            self.n1 = send(self.block(1, 1), self.b1.at[1], self.plus)
            self.n0 = send(self.block(3, 0), self.b0.at[1], self.minus)

        def middle(self):
            self.a0.wait_recv()
            self.c0[...] = (self.b0[0].astype(F32) + self.load(1, 0).astype(F32)).astype(BF16)
            self.e0 = send(self.c0, self.b0.at[2], self.plus)
            self.a1.wait_recv()
            self.c1[...] = (self.b1[0].astype(F32) + self.load(3, 1).astype(F32)).astype(BF16)
            self.e1 = send(self.c1, self.b1.at[2], self.minus)

        def end(self, h):
            for c in ((self.n1, self.e1) if h else (self.n0, self.e0)):
                c.wait_recv()
            got = self.b1 if h else self.b0
            return (self.load(0, h).astype(F32) + got[1].astype(F32) + got[2].astype(F32)).astype(BF16)

    class Spread:
        def __init__(self, base, size, cut):
            self.base, self.size, self.cut = base, size, cut

        def rows(self, r, off, n):
            return out.at[pl.ds(aligned(self.base + self.size * lax.rem(z + r, 4) + off, 16), n)]

        def part(self, r, h):
            return self.rows(r, self.cut * h, self.size - self.cut if h else self.cut)

        def start(self, h):
            ref = self.part(0, h)
            if h:
                self.m1 = send(ref, ref, zm)
                self.p1 = send(ref, ref, zp)
            else:
                self.p0 = send(ref, ref, zp)
                self.m0 = send(ref, ref, zm)

        def middle(self):
            self.p0.wait_recv()
            ref = self.part(3, 0)
            self.f0 = send(ref, ref, zp)
            self.m1.wait_recv()
            ref = self.part(1, 1)
            self.f1 = send(ref, ref, zm)

        def end(self):
            for c in (self.m0, self.p1, self.f0, self.f1):
                c.wait_recv()

    def p1(r, h):
        return p.at[r, pl.ds(R1 // 2 * h, R1 // 2)]

    y_first = Ring(p1, lambda r, h: p[r, R1 // 2 * h:R1 // 2 * (h + 1), :],
                   ya.at[0], ya.at[1], ys.at[0], ys.at[1], yp, ym)

    def q1(r, h):
        return pl.ds(aligned(Q1 * lax.rem(z + r, 4) + 80 * h, 16), 64 if h else 80)

    y_then = Ring(lambda r, h: yr.at[q1(r, h)], lambda r, h: yr[q1(r, h), :],
                  za0, za1, zs0, zs1, zp, zm)
    y_out = Spread(0, Q1, 80)

    def q2(r, h):
        return pl.ds(aligned(R1 + Q2 * lax.rem(z + r, 4) + 64 * h, 16), 64)

    z_first = Ring(lambda r, h: p.at[:, q2(r, h)], lambda r, h: p[:, q2(r, h), :],
                   zb0, zb1, zc0, zc1, zp, zm)
    def zh(h):
        return pl.ds(64 * h, 64)
    z_then = Ring(lambda r, h: zr.at[r, zh(h)], lambda r, h: zr[r, zh(h), :],
                  yb0, yb1, yc0, yc1, yp, ym)
    z_out = Spread(R1, Q2, 64)

    for h in (0, 1):
        late(R1 // 2 * h, R1 // 2, xa)
        y_first.far_half(h)
    for r in (2, 1, 3, 0):
        second_part(r)
    z_first.far()
    z_first.near()
    first_part(1)
    first_part(3)
    y_first.near()

    lt[...] = l[0:704, :].T

    def token_grads(rel):
        rows = jnp.concatenate([lt[slot(k, rel):slot(k, rel) + ROWS, :] for k in range(4)], axis=0)
        return nn(rows, w[0:704, :])

    pb[...] = token_grads(1).astype(BF16)
    pair = send(pb, rb, twin)
    s0[...] = token_grads(0)

    y_first.middle()
    z_first.middle()
    pair.wait_recv()
    sb[...] = (s0[...] + rb[...].astype(F32)).astype(BF16)
    chip = {0: 0, 3: 1, 1: 2, 2: 3}
    def xh(r, h):
        return pl.ds(ROWS * chip[r] + 48 * h, 48)
    x_ring = Ring(lambda r, h: sb.at[xh(r, h)], lambda r, h: sb[xh(r, h), :],
                  xr.at[0], xr.at[1], xs.at[0], xs.at[1], xp, xm)
    x_ring.far()
    x_ring.near()
    first_part(0)
    drain(14)

    zr[:, 0:64, :] = z_first.end(0)
    zr[:, 64:128, :] = z_first.end(1)
    z_then.far()
    z_then.near()
    yr[0:R1 // 2, :] = y_first.end(0)
    yr[R1 // 2:R1, :] = y_first.end(1)
    y_then.far()
    y_then.near()
    drain(8)
    x_ring.middle()
    z_then.middle()
    y_then.middle()
    for h in (0, 1):
        out[z_out_rows(z, h), :] = z_then.end(h)
        z_out.start(h)
    for h in (0, 1):
        out[q1(0, h), :] = y_then.end(h)
        y_out.start(h)
    drain(8)
    gi_ref[0:48, :] = x_ring.end(0)
    gi_ref[48:96, :] = x_ring.end(1)
    z_out.middle()
    y_out.middle()
    z_out.end()
    y_out.end()
    drain()


def z_out_rows(z, h):
    return pl.ds(pl.multiple_of(R1 + Q2 * z + 64 * h, 16), 64)


def finish(factor, gi_ref, dw_ref, gi_hbm, og_hbm, ou_hbm, od_hbm, gi, og, ou, od, sems):
    copies = []
    for i, (buf, dst) in enumerate(((gi, gi_hbm), (og, og_hbm), (ou, ou_hbm), (od, od_hbm))):
        if i == 0:
            buf[...] = gi_ref[...]
        else:
            buf[...] = dw_ref[HID * (i - 1):HID * i, :].astype(F32) * factor
        copies.append(pltpu.make_async_copy(buf, dst, sems.at[i]))
        copies[-1].start()
    for c in copies:
        c.wait()


def body(tokens_in, out_grad, gate_weight, up_weight, down_weight):
    factor = (ROWS * 128) ** (-0.5)
    vmem = pl.BlockSpec(memory_space=pltpu.VMEM)
    hbm = pl.BlockSpec(memory_space=pl.ANY)
    grad_in, sums = pl.pallas_call(
        kernel,
        name="ffn_backward",
        out_shape=(pltpu.VMEM((ROWS, WIDTH), BF16), pltpu.VMEM((RP, SHARD), BF16)),
        in_specs=[pl.BlockSpec(memory_space=pl.ANY)] * 5,
        out_specs=(vmem, vmem),
        scratch_shapes=[
            pltpu.VMEM((TOK, WIDTH), BF16),
            pltpu.VMEM((TOK, WIDTH), BF16),
            pltpu.VMEM((3 * HID, WIDTH), BF16),
            pltpu.VMEM((3 * HID, EARLY), F32),
            pltpu.VMEM((RP, TOK), BF16),
            pltpu.VMEM((TOK, 2 * HID), BF16),
            pltpu.VMEM((R1, SHARD), F32),
            pltpu.VMEM((4, RP, SHARD), BF16),
            pltpu.VMEM((384, WIDTH), BF16),
            pltpu.VMEM((384, WIDTH), BF16),
            pltpu.VMEM((384, WIDTH), F32),
            pltpu.VMEM((384, WIDTH), BF16),
            pltpu.VMEM((2, 3, 48, WIDTH), BF16),
            pltpu.VMEM((2, 48, WIDTH), BF16),
            pltpu.VMEM((2, 3, R1 // 2, SHARD), BF16),
            pltpu.VMEM((2, R1 // 2, SHARD), BF16),
            pltpu.VMEM((R1, SHARD), BF16),
            pltpu.VMEM((3, 80, SHARD), BF16),
            pltpu.VMEM((3, 64, SHARD), BF16),
            pltpu.VMEM((80, SHARD), BF16),
            pltpu.VMEM((64, SHARD), BF16),
            pltpu.VMEM((3, 4, 64, SHARD), BF16),
            pltpu.VMEM((3, 4, 64, SHARD), BF16),
            pltpu.VMEM((4, 64, SHARD), BF16),
            pltpu.VMEM((4, 64, SHARD), BF16),
            pltpu.VMEM((4, Q2, SHARD), BF16),
            pltpu.VMEM((3, 64, SHARD), BF16),
            pltpu.VMEM((3, 64, SHARD), BF16),
            pltpu.VMEM((64, SHARD), BF16),
            pltpu.VMEM((64, SHARD), BF16),
            pltpu.SemaphoreType.DMA((5,)),
            pltpu.SemaphoreType.DMA((96,)),
            pltpu.SemaphoreType.DMA((96,)),
        ],
        compiler_params=pltpu.CompilerParams(collective_id=0, has_side_effects=True),
    )(tokens_in, out_grad, gate_weight.T, up_weight.T, down_weight)
    grad_in, gg, gu, gd = pl.pallas_call(
        functools.partial(finish, factor),
        name="finish",
        out_shape=(jax.ShapeDtypeStruct((ROWS, WIDTH), BF16),) + (jax.ShapeDtypeStruct((HID, SHARD), F32),) * 3,
        in_specs=[vmem, vmem],
        out_specs=(hbm,) * 4,
        scratch_shapes=[pltpu.VMEM((ROWS, WIDTH), BF16)] + [pltpu.VMEM((HID, SHARD), F32)] * 3
        + [pltpu.SemaphoreType.DMA((4,))],
        compiler_params=pltpu.CompilerParams(vmem_limit_bytes=8 << 20),
    )(grad_in, sums)
    return grad_in, gg.T, gu.T, gd


def solution(mesh):
    return jax.shard_map(
        body,
        mesh=mesh,
        in_specs=(
            P(("rep", "fs", "tp"), None),
            P(("rep", "fs", "tp"), None),
            P("fs", "tp"),
            P("fs", "tp"),
            P("tp", "fs"),
        ),
        out_specs=(P(("rep", "fs", "tp"), None), P("fs", "tp"), P("fs", "tp"), P("tp", "fs")),
        check_vma=False,
    )
```

```python
import functools

import jax
import jax.numpy as jnp
from jax import lax
from jax.experimental import pallas as pl
from jax.experimental.pallas import tpu as pltpu
from jax.sharding import PartitionSpec as P

MESH = pl.DeviceIdType.MESH
F32 = jnp.float32
BF16 = jnp.bfloat16

ROWS = 96
WIDTH = 1024
HID = 352
SHARD = 256
TOK = 768
EARLY = 512
R1 = 640
R2 = 448
RP = R1 + R2
PIECE, Q2 = R1 // 4, R2 // 4


def nt(a, b):
    return lax.dot_general(a, b, (((1,), (1,)), ((), ())), preferred_element_type=F32)


def nn(a, b):
    return lax.dot_general(a, b, (((1,), (0,)), ((), ())), preferred_element_type=F32)


def aligned(value, by):
    return pl.multiple_of(value, by)


def kernel(x_hbm, o_hbm, g_hbm, u_hbm, d_hbm, gi_ref, out,
           xa, oa, w, fwd, l, lt, pa, p, pb, rb, s0, sb, xr, xs,
           ya, ys, yr, got, half_sum, zb0, zb1, zc0, zc1, zr, yb0, yb1, yc0, yc1,
           ls, ss, rs):
    z = lax.axis_index("rep")
    y = lax.axis_index("fs")
    t = lax.axis_index("tp")
    core = lax.rem(t, 2)
    half = lax.rem(z, 2)
    xp = (z, y, lax.rem(t + 2, 8))
    xm = (z, y, lax.rem(t + 6, 8))
    twin = (z, y, t + 1 - 2 * core)
    yp = (z, lax.rem(y + 1, 4), t)
    ym = (z, lax.rem(y + 3, 4), t)
    zp = (lax.rem(z + 1, 4), y, t)
    zm = (lax.rem(z + 3, 4), y, t)

    counter = [0]
    started = []

    def send(src, dst, dev):
        i = counter[0]
        counter[0] += 1
        copy = pltpu.make_async_remote_copy(
            src_ref=src, dst_ref=dst, send_sem=ss.at[i], recv_sem=rs.at[i],
            device_id=dev, device_id_type=MESH)
        copy.start()
        started.append(copy)
        return copy

    def drain(keep=0):
        while len(started) > keep:
            started.pop(0).wait_send()

    mine = pl.ds(aligned(y * SHARD, SHARD), SHARD)
    locals_ = [
        pltpu.make_async_copy(x_hbm, xa.at[pl.ds(0, ROWS)], ls.at[0]),
        pltpu.make_async_copy(g_hbm, w.at[pl.ds(0, HID), mine], ls.at[1]),
        pltpu.make_async_copy(u_hbm, w.at[pl.ds(HID, HID), mine], ls.at[2]),
        pltpu.make_async_copy(d_hbm, w.at[pl.ds(2 * HID, HID), mine], ls.at[3]),
        pltpu.make_async_copy(o_hbm, oa.at[pl.ds(0, ROWS)], ls.at[4]),
    ]
    for c in locals_:
        c.start()

    barrier = pltpu.get_barrier_semaphore()
    for dev in (xp, xm, twin, yp, ym, zp, zm):
        pl.semaphore_signal(barrier, inc=1, device_id=dev, device_id_type=MESH)
    l[pl.ds(3 * HID, RP - 3 * HID), :] = jnp.zeros((RP - 3 * HID, TOK), BF16)
    pl.semaphore_wait(barrier, 7)

    def slot(k, rel):
        return 2 * ROWS * k + ROWS * rel

    def tok(ref, row, n):
        return ref.at[pl.ds(row, n)]

    my_rows = [aligned(640 * half, 16), aligned(640 * half + 208, 16), 416]

    def wblk(row, n, col):
        return w.at[pl.ds(row, n), pl.ds(aligned(lax.rem(col, 4) * SHARD, SHARD), SHARD)]

    def wsend(i, off, n, col, dev):
        ref = wblk(my_rows[i] + off if off else my_rows[i], n, col)
        return send(ref, ref, dev)

    for c in locals_[:1]:
        c.wait()
    x_p = send(tok(xa, 0, ROWS), tok(xa, slot(1, 0), ROWS), xp)
    x_m = send(tok(xa, 0, ROWS), tok(xa, slot(2, 0), ROWS), xm)
    x_t = send(tok(xa, 0, ROWS), tok(xa, slot(0, 1), ROWS), twin)
    for c in locals_[1:4]:
        c.wait()
    wp_a = wsend(0, 0, 208, y, yp)
    wm_b = wsend(1, 0, 208, y, ym)
    wp_b = wsend(1, 0, 208, y, yp)
    wm_a = wsend(0, 0, 208, y, ym)
    locals_[4].wait()
    o_p = send(tok(oa, 0, ROWS), tok(oa, slot(1, 0), ROWS), xp)
    o_m = send(tok(oa, 0, ROWS), tok(oa, slot(2, 0), ROWS), xm)
    o_t = send(tok(oa, 0, ROWS), tok(oa, slot(0, 1), ROWS), twin)

    z_in = []

    def zsend(i, col, dev):
        z_in.append(wsend(i, 0, 208, col, dev))

    wp_a.wait_recv()
    fp_a = wsend(0, 0, 208, y + 3, yp)
    zsend(0, y + 3, zp)
    wm_b.wait_recv()
    fm_b = wsend(1, 0, 208, y + 1, ym)
    zsend(1, y + 1, zm)
    wp_c = wsend(2, 0, 224, y, yp)
    wm_c = wsend(2, 0, 224, y, ym)

    x_p.wait_recv()
    xf_p = send(tok(xa, slot(1, 0), 48), tok(xa, slot(3, 0), 48), xp)
    x_m.wait_recv()
    xf_m = send(tok(xa, slot(2, 0) + 48, 48), tok(xa, slot(3, 0) + 48, 48), xm)
    xt1 = send(tok(xa, slot(1, 0), ROWS), tok(xa, slot(1, 1), ROWS), twin)
    xt2 = send(tok(xa, slot(2, 0), ROWS), tok(xa, slot(2, 1), ROWS), twin)

    wp_b.wait_recv()
    zsend(1, y + 3, zm)
    wm_a.wait_recv()
    zsend(0, y + 1, zp)
    fp_a.wait_recv()
    zsend(0, y + 2, zp)
    fm_b.wait_recv()
    zsend(1, y + 2, zm)

    wp_c.wait_recv()
    fp_c = wsend(2, 0, 112, y + 3, yp)
    wm_c.wait_recv()
    fm_c = wsend(2, 112, 112, y + 1, ym)

    o_p.wait_recv()
    of_p = send(tok(oa, slot(1, 0), 48), tok(oa, slot(3, 0), 48), xp)
    o_m.wait_recv()
    of_m = send(tok(oa, slot(2, 0) + 48, 48), tok(oa, slot(3, 0) + 48, 48), xm)
    ot1 = send(tok(oa, slot(1, 0), ROWS), tok(oa, slot(1, 1), ROWS), twin)
    ot2 = send(tok(oa, slot(2, 0), ROWS), tok(oa, slot(2, 1), ROWS), twin)

    xf_p.wait_recv()
    xt3 = send(tok(xa, slot(3, 0), 48), tok(xa, slot(3, 1), 48), twin)
    xf_m.wait_recv()
    xt4 = send(tok(xa, slot(3, 0) + 48, 48), tok(xa, slot(3, 1) + 48, 48), twin)
    for c in (fp_c, fm_c):
        c.wait_recv()
    for c in z_in:
        c.wait_recv()
    for c in (x_t, o_t, xt1, xt2, ot1, ot2):
        c.wait_recv()

    def project(c0, n, parts=(0, 1, 2)):
        cols = pl.ds(c0, n)
        for part in parts:
            source = oa if part == 2 else xa
            rows = pl.ds(HID * part, HID)
            fwd[rows, cols] = nt(w[rows, :], source[cols, :])

    def elementwise(c0, n):
        cols = pl.ds(c0, n)
        for m in range(11):
            a = 32 * m
            g = fwd[a:a + 32, cols].astype(BF16).astype(F32)
            u = fwd[HID + a:HID + a + 32, cols].astype(BF16).astype(F32)
            gh = fwd[2 * HID + a:2 * HID + a + 32, cols].astype(BF16).astype(F32)
            sig = 1.0 / (1.0 + jnp.exp(-g))
            act = g * sig
            l[a:a + 32, cols] = (gh * u * sig * (1.0 + g * (1.0 - sig))).astype(BF16)
            l[HID + a:HID + a + 32, cols] = (gh * act).astype(BF16)
            l[2 * HID + a:2 * HID + a + 32, cols] = (act * u).astype(BF16)

    def shard_cols(r):
        return pl.ds(aligned(lax.rem(y + r, 4) * SHARD, SHARD), SHARD)

    def early(row, n, source):
        pa[row:row + n, :] = nn(l[row:row + n, 0:EARLY], source[0:EARLY, shard_cols(2)])

    def late(row, n, source):
        more = nn(l[row:row + n, EARLY:TOK], source[EARLY:TOK, shard_cols(2)])
        p[2, row:row + n, :] = (pa[row:row + n, :] + more).astype(BF16)

    def whole(r, row, n, source):
        p[r, row:row + n, :] = nn(l[row:row + n, :], source[:, shard_cols(r)]).astype(BF16)

    def first_part(r):
        whole(r, 0, R1 // 2, xa)
        whole(r, R1 // 2, R1 // 2, xa)

    def second_part(r):
        whole(r, R1, 704 - R1, xa)
        whole(r, 704, RP - 704, oa)

    project(0, 256)
    elementwise(0, 256)
    of_p.wait_recv()
    ot3 = send(tok(oa, slot(3, 0), 48), tok(oa, slot(3, 1), 48), twin)
    of_m.wait_recv()
    ot4 = send(tok(oa, slot(3, 0) + 48, 48), tok(oa, slot(3, 1) + 48, 48), twin)
    project(256, EARLY - 256)
    elementwise(256, EARLY - 256)
    xt3.wait_recv()
    xt4.wait_recv()
    project(EARLY, TOK - EARLY, (0, 1))
    early(0, R1 // 2, xa)
    early(R1 // 2, R1 // 2, xa)
    ot3.wait_recv()
    ot4.wait_recv()
    project(EARLY, TOK - EARLY, (2,))
    elementwise(EARLY, TOK - EARLY)

    class Ring:
        def __init__(self, block, load, b0, b1, c0, c1, plus, minus):
            self.block, self.load = block, load
            self.b0, self.b1, self.c0, self.c1 = b0, b1, c0, c1
            self.plus, self.minus = plus, minus

        def far(self):
            self.far_half(0)
            self.far_half(1)

        def far_half(self, h):
            if h:
                self.a1 = send(self.block(2, 1), self.b1.at[0], self.minus)
            else:
                self.a0 = send(self.block(2, 0), self.b0.at[0], self.plus)

        def near(self):
            self.n1 = send(self.block(1, 1), self.b1.at[1], self.plus)
            self.n0 = send(self.block(3, 0), self.b0.at[1], self.minus)

        def middle(self):
            self.a0.wait_recv()
            self.c0[...] = (self.b0[0].astype(F32) + self.load(1, 0).astype(F32)).astype(BF16)
            self.e0 = send(self.c0, self.b0.at[2], self.plus)
            self.a1.wait_recv()
            self.c1[...] = (self.b1[0].astype(F32) + self.load(3, 1).astype(F32)).astype(BF16)
            self.e1 = send(self.c1, self.b1.at[2], self.minus)

        def end(self, h):
            for c in ((self.n1, self.e1) if h else (self.n0, self.e0)):
                c.wait_recv()
            got = self.b1 if h else self.b0
            return (self.load(0, h).astype(F32) + got[1].astype(F32) + got[2].astype(F32)).astype(BF16)

    class Spread:
        def __init__(self, base, size, cut):
            self.base, self.size, self.cut = base, size, cut

        def rows(self, r, off, n):
            return out.at[pl.ds(aligned(self.base + self.size * lax.rem(z + r, 4) + off, 16), n)]

        def part(self, r, h):
            return self.rows(r, self.cut * h, self.size - self.cut if h else self.cut)

        def start(self, h):
            ref = self.part(0, h)
            if h:
                self.m1 = send(ref, ref, zm)
                self.p1 = send(ref, ref, zp)
            else:
                self.p0 = send(ref, ref, zp)
                self.m0 = send(ref, ref, zm)

        def middle(self):
            self.p0.wait_recv()
            ref = self.part(3, 0)
            self.f0 = send(ref, ref, zp)
            self.m1.wait_recv()
            ref = self.part(1, 1)
            self.f1 = send(ref, ref, zm)

        def end(self):
            for c in (self.m0, self.p1, self.f0, self.f1):
                c.wait_recv()

    def p1(r, h):
        return p.at[r, pl.ds(R1 // 2 * h, R1 // 2)]

    y_first = Ring(p1, lambda r, h: p[r, R1 // 2 * h:R1 // 2 * (h + 1), :],
                   ya.at[0], ya.at[1], ys.at[0], ys.at[1], yp, ym)

    pair_a = (z + 1 - 2 * half, y, t)
    pair_b = (lax.rem(z + 3 + 2 * half, 4), y, t)

    class Exchange:
        def __init__(self, i):
            self.i, self.rows = i, pl.ds(PIECE * i, PIECE)
            self.first, self.second = (pair_a, pair_b) if i < 2 else (pair_b, pair_a)

        def start(self):
            self.c0 = send(yr.at[self.rows], got.at[0, self.rows], self.first)

        def middle(self):
            self.c0.wait_recv()
            half_sum[self.rows, :] = (yr[self.rows, :].astype(F32) + got[0, self.rows, :].astype(F32)).astype(BF16)
            self.c1 = send(half_sum.at[self.rows], got.at[1, self.rows], self.second)

        def end(self):
            self.c1.wait_recv()
            out[self.rows, :] = (half_sum[self.rows, :].astype(F32) + got[1, self.rows, :].astype(F32)).astype(BF16)

    swaps = [Exchange(i) for i in range(4)]

    def q2(r, h):
        return pl.ds(aligned(R1 + Q2 * lax.rem(z + r, 4) + 64 * h, 16), 48 if h else 64)

    z_first = Ring(lambda r, h: p.at[:, q2(r, h)], lambda r, h: p[:, q2(r, h), :],
                   zb0, zb1, zc0, zc1, zp, zm)
    def zh(h):
        return pl.ds(64 * h, 48 if h else 64)
    z_then = Ring(lambda r, h: zr.at[r, zh(h)], lambda r, h: zr[r, zh(h), :],
                  yb0, yb1, yc0, yc1, yp, ym)
    z_out = Spread(R1, Q2, 64)

    for h in (0, 1):
        late(R1 // 2 * h, R1 // 2, xa)
        y_first.far_half(h)
    for r in (2, 1, 3, 0):
        second_part(r)
    z_first.far()
    z_first.near()
    first_part(1)
    first_part(3)
    y_first.near()

    lt[...] = l[0:704, :].T

    def token_grads(rel):
        rows = jnp.concatenate([lt[slot(k, rel):slot(k, rel) + ROWS, :] for k in range(4)], axis=0)
        return nn(rows, w[0:704, :])

    pb[...] = token_grads(1).astype(BF16)
    pair = send(pb, rb, twin)
    s0[...] = token_grads(0)

    y_first.middle()
    z_first.middle()
    pair.wait_recv()
    sb[...] = (s0[...] + rb[...].astype(F32)).astype(BF16)
    chip = {0: 0, 3: 1, 1: 2, 2: 3}
    def xh(r, h):
        return pl.ds(ROWS * chip[r] + 48 * h, 48)
    x_ring = Ring(lambda r, h: sb.at[xh(r, h)], lambda r, h: sb[xh(r, h), :],
                  xr.at[0], xr.at[1], xs.at[0], xs.at[1], xp, xm)
    x_ring.far()
    x_ring.near()
    first_part(0)
    drain(14)

    zr[:, 0:64, :] = z_first.end(0)
    zr[:, 64:112, :] = z_first.end(1)
    z_then.far()
    z_then.near()
    yr[0:R1 // 2, :] = y_first.end(0)
    swaps[0].start()
    swaps[1].start()
    yr[R1 // 2:R1, :] = y_first.end(1)
    swaps[2].start()
    swaps[3].start()
    drain(8)
    x_ring.middle()
    z_then.middle()
    for i in (0, 2):
        swaps[i].middle()
    for h in (0, 1):
        out[z_out_rows(z, h), :] = z_then.end(h)
        z_out.start(h)
    for i in (1, 3):
        swaps[i].middle()
    drain(8)
    gi_ref[0:48, :] = x_ring.end(0)
    gi_ref[48:96, :] = x_ring.end(1)
    z_out.middle()
    for i in (0, 2, 1, 3):
        swaps[i].end()
    z_out.end()
    drain()


def z_out_rows(z, h):
    return pl.ds(pl.multiple_of(R1 + Q2 * z + 64 * h, 16), 48 if h else 64)


def finish(factor, gi_ref, dw_ref, gi_hbm, og_hbm, ou_hbm, od_hbm, gi, og, ou, od, sems):
    copies = []
    for i, (buf, dst) in enumerate(((gi, gi_hbm), (og, og_hbm), (ou, ou_hbm), (od, od_hbm))):
        if i == 0:
            buf[...] = gi_ref[...]
        else:
            buf[...] = dw_ref[HID * (i - 1):HID * i, :].astype(F32) * factor
        copies.append(pltpu.make_async_copy(buf, dst, sems.at[i]))
        copies[-1].start()
    for c in copies:
        c.wait()


def body(tokens_in, out_grad, gate_weight, up_weight, down_weight):
    factor = (ROWS * 128) ** (-0.5)
    vmem = pl.BlockSpec(memory_space=pltpu.VMEM)
    hbm = pl.BlockSpec(memory_space=pl.ANY)
    grad_in, sums = pl.pallas_call(
        kernel,
        name="ffn_backward",
        out_shape=(pltpu.VMEM((ROWS, WIDTH), BF16), pltpu.VMEM((RP, SHARD), BF16)),
        in_specs=[pl.BlockSpec(memory_space=pl.ANY)] * 5,
        out_specs=(vmem, vmem),
        scratch_shapes=[
            pltpu.VMEM((TOK, WIDTH), BF16),
            pltpu.VMEM((TOK, WIDTH), BF16),
            pltpu.VMEM((3 * HID, WIDTH), BF16),
            pltpu.VMEM((3 * HID, TOK), F32),
            pltpu.VMEM((RP, TOK), BF16),
            pltpu.VMEM((TOK, 2 * HID), BF16),
            pltpu.VMEM((R1, SHARD), F32),
            pltpu.VMEM((4, RP, SHARD), BF16),
            pltpu.VMEM((384, WIDTH), BF16),
            pltpu.VMEM((384, WIDTH), BF16),
            pltpu.VMEM((384, WIDTH), F32),
            pltpu.VMEM((384, WIDTH), BF16),
            pltpu.VMEM((2, 3, 48, WIDTH), BF16),
            pltpu.VMEM((2, 48, WIDTH), BF16),
            pltpu.VMEM((2, 3, R1 // 2, SHARD), BF16),
            pltpu.VMEM((2, R1 // 2, SHARD), BF16),
            pltpu.VMEM((R1, SHARD), BF16),
            pltpu.VMEM((2, R1, SHARD), BF16),
            pltpu.VMEM((R1, SHARD), BF16),
            pltpu.VMEM((3, 4, 64, SHARD), BF16),
            pltpu.VMEM((3, 4, 48, SHARD), BF16),
            pltpu.VMEM((4, 64, SHARD), BF16),
            pltpu.VMEM((4, 48, SHARD), BF16),
            pltpu.VMEM((4, Q2, SHARD), BF16),
            pltpu.VMEM((3, 64, SHARD), BF16),
            pltpu.VMEM((3, 48, SHARD), BF16),
            pltpu.VMEM((64, SHARD), BF16),
            pltpu.VMEM((48, SHARD), BF16),
            pltpu.SemaphoreType.DMA((5,)),
            pltpu.SemaphoreType.DMA((96,)),
            pltpu.SemaphoreType.DMA((96,)),
        ],
        compiler_params=pltpu.CompilerParams(collective_id=0, has_side_effects=True),
    )(tokens_in, out_grad, gate_weight.T, up_weight.T, down_weight)
    grad_in, gg, gu, gd = pl.pallas_call(
        functools.partial(finish, factor),
        name="finish",
        out_shape=(jax.ShapeDtypeStruct((ROWS, WIDTH), BF16),) + (jax.ShapeDtypeStruct((HID, SHARD), F32),) * 3,
        in_specs=[vmem, vmem],
        out_specs=(hbm,) * 4,
        scratch_shapes=[pltpu.VMEM((ROWS, WIDTH), BF16)] + [pltpu.VMEM((HID, SHARD), F32)] * 3
        + [pltpu.SemaphoreType.DMA((4,))],
        compiler_params=pltpu.CompilerParams(vmem_limit_bytes=8 << 20),
    )(grad_in, sums)
    return grad_in, gg.T, gu.T, gd


def solution(mesh):
    return jax.shard_map(
        body,
        mesh=mesh,
        in_specs=(
            P(("rep", "fs", "tp"), None),
            P(("rep", "fs", "tp"), None),
            P("fs", "tp"),
            P("fs", "tp"),
            P("tp", "fs"),
        ),
        out_specs=(P(("rep", "fs", "tp"), None), P("fs", "tp"), P("fs", "tp"), P("tp", "fs")),
        check_vma=False,
    )
```

```python
import functools

import jax
import jax.numpy as jnp
from jax import lax
from jax.experimental import pallas as pl
from jax.experimental.pallas import tpu as pltpu
from jax.sharding import PartitionSpec as P

MESH = pl.DeviceIdType.MESH
F32 = jnp.float32
BF16 = jnp.bfloat16

ROWS = 96
WIDTH = 1024
HID = 352
SHARD = 256
TOK = 768
EARLY = 512
R1 = 576
R2 = 512
RP = R1 + R2
PIECE, Q2 = R1 // 4, R2 // 4
H0, H1 = 64, 64


def nt(a, b):
    return lax.dot_general(a, b, (((1,), (1,)), ((), ())), preferred_element_type=F32)


def nn(a, b):
    return lax.dot_general(a, b, (((1,), (0,)), ((), ())), preferred_element_type=F32)


def aligned(value, by):
    return pl.multiple_of(value, by)


def kernel(x_hbm, o_hbm, g_hbm, u_hbm, d_hbm, gi_ref, out,
           xa, oa, w, fwd, l, lt, pa, pz, p, pb, rb, s0, sb, xr, xs,
           ya, ys, yr, got, half_sum, zb0, zb1, zc0, zc1, zr, yb0, yb1, yc0, yc1,
           ls, ss, rs):
    z = lax.axis_index("rep")
    y = lax.axis_index("fs")
    t = lax.axis_index("tp")
    core = lax.rem(t, 2)
    half = lax.rem(z, 2)
    xp = (z, y, lax.rem(t + 2, 8))
    xm = (z, y, lax.rem(t + 6, 8))
    twin = (z, y, t + 1 - 2 * core)
    yp = (z, lax.rem(y + 1, 4), t)
    ym = (z, lax.rem(y + 3, 4), t)
    zp = (lax.rem(z + 1, 4), y, t)
    zm = (lax.rem(z + 3, 4), y, t)

    counter = [0]
    started = []

    def send(src, dst, dev):
        i = counter[0]
        counter[0] += 1
        copy = pltpu.make_async_remote_copy(
            src_ref=src, dst_ref=dst, send_sem=ss.at[i], recv_sem=rs.at[i],
            device_id=dev, device_id_type=MESH)
        copy.start()
        started.append(copy)
        return copy

    def drain(keep=0):
        while len(started) > keep:
            started.pop(0).wait_send()

    mine = pl.ds(aligned(y * SHARD, SHARD), SHARD)
    locals_ = [
        pltpu.make_async_copy(x_hbm, xa.at[pl.ds(0, ROWS)], ls.at[0]),
        pltpu.make_async_copy(g_hbm, w.at[pl.ds(0, HID), mine], ls.at[1]),
        pltpu.make_async_copy(u_hbm, w.at[pl.ds(HID, HID), mine], ls.at[2]),
        pltpu.make_async_copy(d_hbm, w.at[pl.ds(2 * HID, HID), mine], ls.at[3]),
        pltpu.make_async_copy(o_hbm, oa.at[pl.ds(0, ROWS)], ls.at[4]),
    ]
    for c in locals_:
        c.start()

    barrier = pltpu.get_barrier_semaphore()
    for dev in (xp, xm, twin, yp, ym, zp, zm):
        pl.semaphore_signal(barrier, inc=1, device_id=dev, device_id_type=MESH)
    l[pl.ds(3 * HID, RP - 3 * HID), :] = jnp.zeros((RP - 3 * HID, TOK), BF16)
    pl.semaphore_wait(barrier, 7)

    def slot(k, rel):
        return 2 * ROWS * k + ROWS * rel

    def tok(ref, row, n):
        return ref.at[pl.ds(row, n)]

    my_rows = [aligned(640 * half, 16), aligned(640 * half + 208, 16), 416]

    def wblk(row, n, col):
        return w.at[pl.ds(row, n), pl.ds(aligned(lax.rem(col, 4) * SHARD, SHARD), SHARD)]

    def wsend(i, off, n, col, dev):
        ref = wblk(my_rows[i] + off if off else my_rows[i], n, col)
        return send(ref, ref, dev)

    for c in locals_[:1]:
        c.wait()
    x_p = send(tok(xa, 0, ROWS), tok(xa, slot(1, 0), ROWS), xp)
    x_m = send(tok(xa, 0, ROWS), tok(xa, slot(2, 0), ROWS), xm)
    x_t = send(tok(xa, 0, ROWS), tok(xa, slot(0, 1), ROWS), twin)
    for c in locals_[1:4]:
        c.wait()
    wp_a = wsend(0, 0, 208, y, yp)
    wm_b = wsend(1, 0, 208, y, ym)
    wp_b = wsend(1, 0, 208, y, yp)
    wm_a = wsend(0, 0, 208, y, ym)
    locals_[4].wait()
    o_p = send(tok(oa, 0, ROWS), tok(oa, slot(1, 0), ROWS), xp)
    o_m = send(tok(oa, 0, ROWS), tok(oa, slot(2, 0), ROWS), xm)
    o_t = send(tok(oa, 0, ROWS), tok(oa, slot(0, 1), ROWS), twin)

    z_in = []

    def zsend(i, col, dev):
        z_in.append(wsend(i, 0, 208, col, dev))

    wp_a.wait_recv()
    fp_a = wsend(0, 0, 208, y + 3, yp)
    zsend(0, y + 3, zp)
    wm_b.wait_recv()
    fm_b = wsend(1, 0, 208, y + 1, ym)
    zsend(1, y + 1, zm)
    wp_c = wsend(2, 0, 224, y, yp)
    wm_c = wsend(2, 0, 224, y, ym)

    x_p.wait_recv()
    xf_p = send(tok(xa, slot(1, 0), 48), tok(xa, slot(3, 0), 48), xp)
    x_m.wait_recv()
    xf_m = send(tok(xa, slot(2, 0) + 48, 48), tok(xa, slot(3, 0) + 48, 48), xm)
    xt1 = send(tok(xa, slot(1, 0), ROWS), tok(xa, slot(1, 1), ROWS), twin)
    xt2 = send(tok(xa, slot(2, 0), ROWS), tok(xa, slot(2, 1), ROWS), twin)

    wp_b.wait_recv()
    zsend(1, y + 3, zm)
    wm_a.wait_recv()
    zsend(0, y + 1, zp)
    fp_a.wait_recv()
    zsend(0, y + 2, zp)
    fm_b.wait_recv()
    zsend(1, y + 2, zm)

    wp_c.wait_recv()
    fp_c = wsend(2, 0, 112, y + 3, yp)
    wm_c.wait_recv()
    fm_c = wsend(2, 112, 112, y + 1, ym)

    o_p.wait_recv()
    of_p = send(tok(oa, slot(1, 0), 48), tok(oa, slot(3, 0), 48), xp)
    o_m.wait_recv()
    of_m = send(tok(oa, slot(2, 0) + 48, 48), tok(oa, slot(3, 0) + 48, 48), xm)
    ot1 = send(tok(oa, slot(1, 0), ROWS), tok(oa, slot(1, 1), ROWS), twin)
    ot2 = send(tok(oa, slot(2, 0), ROWS), tok(oa, slot(2, 1), ROWS), twin)

    xf_p.wait_recv()
    xt3 = send(tok(xa, slot(3, 0), 48), tok(xa, slot(3, 1), 48), twin)
    xf_m.wait_recv()
    xt4 = send(tok(xa, slot(3, 0) + 48, 48), tok(xa, slot(3, 1) + 48, 48), twin)
    for c in (fp_c, fm_c):
        c.wait_recv()
    for c in z_in:
        c.wait_recv()
    for c in (x_t, o_t, xt1, xt2, ot1, ot2):
        c.wait_recv()

    def project(c0, n, parts=(0, 1, 2)):
        cols = pl.ds(c0, n)
        for part in parts:
            source = oa if part == 2 else xa
            rows = pl.ds(HID * part, HID)
            fwd[rows, cols] = nt(w[rows, :], source[cols, :])

    def elementwise(c0, n):
        cols = pl.ds(c0, n)
        for m in range(11):
            a = 32 * m
            g = fwd[a:a + 32, cols].astype(BF16).astype(F32)
            u = fwd[HID + a:HID + a + 32, cols].astype(BF16).astype(F32)
            gh = fwd[2 * HID + a:2 * HID + a + 32, cols].astype(BF16).astype(F32)
            sig = 1.0 / (1.0 + jnp.exp(-g))
            act = g * sig
            l[a:a + 32, cols] = (gh * u * sig * (1.0 + g * (1.0 - sig))).astype(BF16)
            l[HID + a:HID + a + 32, cols] = (gh * act).astype(BF16)
            l[2 * HID + a:2 * HID + a + 32, cols] = (act * u).astype(BF16)

    def shard_cols(r):
        return pl.ds(aligned(lax.rem(y + r, 4) * SHARD, SHARD), SHARD)

    def early(row, n, source):
        pa[row:row + n, :] = nn(l[row:row + n, 0:EARLY], source[0:EARLY, shard_cols(2)])

    def late(row, n, source):
        more = nn(l[row:row + n, EARLY:TOK], source[EARLY:TOK, shard_cols(2)])
        p[2, row:row + n, :] = (pa[row:row + n, :] + more).astype(BF16)

    def whole(r, row, n, source):
        p[r, row:row + n, :] = nn(l[row:row + n, :], source[:, shard_cols(r)]).astype(BF16)

    def early_second(r):
        pz[r, 0:704 - R1, :] = nn(l[R1:704, 0:EARLY], xa[0:EARLY, shard_cols(r)])
        pz[r, 704 - R1:R2, :] = nn(l[704:RP, 0:EARLY], oa[0:EARLY, shard_cols(r)])

    def first_part(r):
        whole(r, 0, R1 // 2, xa)
        whole(r, R1 // 2, R1 // 2, xa)

    def second_part(r):
        more = nn(l[R1:704, EARLY:TOK], xa[EARLY:TOK, shard_cols(r)])
        p[r, R1:704, :] = (pz[r, 0:704 - R1, :] + more).astype(BF16)
        more = nn(l[704:RP, EARLY:TOK], oa[EARLY:TOK, shard_cols(r)])
        p[r, 704:RP, :] = (pz[r, 704 - R1:R2, :] + more).astype(BF16)

    project(0, 256)
    elementwise(0, 256)
    of_p.wait_recv()
    ot3 = send(tok(oa, slot(3, 0), 48), tok(oa, slot(3, 1), 48), twin)
    of_m.wait_recv()
    ot4 = send(tok(oa, slot(3, 0) + 48, 48), tok(oa, slot(3, 1) + 48, 48), twin)
    project(256, EARLY - 256)
    elementwise(256, EARLY - 256)
    xt3.wait_recv()
    xt4.wait_recv()
    project(EARLY, TOK - EARLY, (0, 1))
    early(0, R1 // 2, xa)
    early(R1 // 2, R1 // 2, xa)
    for r in (2, 1, 3, 0):
        early_second(r)
    ot3.wait_recv()
    ot4.wait_recv()
    project(EARLY, TOK - EARLY, (2,))
    elementwise(EARLY, TOK - EARLY)

    class Ring:
        def __init__(self, block, load, b0, b1, c0, c1, plus, minus):
            self.block, self.load = block, load
            self.b0, self.b1, self.c0, self.c1 = b0, b1, c0, c1
            self.plus, self.minus = plus, minus

        def far(self):
            self.far_half(0)
            self.far_half(1)

        def far_half(self, h):
            if h:
                self.a1 = send(self.block(2, 1), self.b1.at[0], self.minus)
            else:
                self.a0 = send(self.block(2, 0), self.b0.at[0], self.plus)

        def near(self):
            self.n1 = send(self.block(1, 1), self.b1.at[1], self.plus)
            self.n0 = send(self.block(3, 0), self.b0.at[1], self.minus)

        def middle(self):
            self.a0.wait_recv()
            self.c0[...] = (self.b0[0].astype(F32) + self.load(1, 0).astype(F32)).astype(BF16)
            self.e0 = send(self.c0, self.b0.at[2], self.plus)
            self.a1.wait_recv()
            self.c1[...] = (self.b1[0].astype(F32) + self.load(3, 1).astype(F32)).astype(BF16)
            self.e1 = send(self.c1, self.b1.at[2], self.minus)

        def end(self, h):
            for c in ((self.n1, self.e1) if h else (self.n0, self.e0)):
                c.wait_recv()
            got = self.b1 if h else self.b0
            return (self.load(0, h).astype(F32) + got[1].astype(F32) + got[2].astype(F32)).astype(BF16)

    class Spread:
        def __init__(self, base, size, cut):
            self.base, self.size, self.cut = base, size, cut

        def rows(self, r, off, n):
            return out.at[pl.ds(aligned(self.base + self.size * lax.rem(z + r, 4) + off, 16), n)]

        def part(self, r, h):
            return self.rows(r, self.cut * h, self.size - self.cut if h else self.cut)

        def start(self, h):
            ref = self.part(0, h)
            if h:
                self.m1 = send(ref, ref, zm)
                self.p1 = send(ref, ref, zp)
            else:
                self.p0 = send(ref, ref, zp)
                self.m0 = send(ref, ref, zm)

        def middle(self):
            self.p0.wait_recv()
            ref = self.part(3, 0)
            self.f0 = send(ref, ref, zp)
            self.m1.wait_recv()
            ref = self.part(1, 1)
            self.f1 = send(ref, ref, zm)

        def end(self):
            for c in (self.m0, self.p1, self.f0, self.f1):
                c.wait_recv()

    def p1(r, h):
        return p.at[r, pl.ds(R1 // 2 * h, R1 // 2)]

    y_first = Ring(p1, lambda r, h: p[r, R1 // 2 * h:R1 // 2 * (h + 1), :],
                   ya.at[0], ya.at[1], ys.at[0], ys.at[1], yp, ym)

    pair_a = (z + 1 - 2 * half, y, t)
    pair_b = (lax.rem(z + 3 + 2 * half, 4), y, t)

    class Exchange:
        def __init__(self, i):
            self.i, self.rows = i, pl.ds(PIECE * i, PIECE)
            self.first, self.second = (pair_a, pair_b) if i < 2 else (pair_b, pair_a)

        def start(self):
            self.c0 = send(yr.at[self.rows], got.at[0, self.rows], self.first)

        def middle(self):
            self.c0.wait_recv()
            half_sum[self.rows, :] = (yr[self.rows, :].astype(F32) + got[0, self.rows, :].astype(F32)).astype(BF16)
            self.c1 = send(half_sum.at[self.rows], got.at[1, self.rows], self.second)

        def end(self):
            self.c1.wait_recv()
            out[self.rows, :] = (half_sum[self.rows, :].astype(F32) + got[1, self.rows, :].astype(F32)).astype(BF16)

    swaps = [Exchange(i) for i in range(4)]

    def q2(r, h):
        return pl.ds(aligned(R1 + Q2 * lax.rem(z + r, 4) + H0 * h, 16), H1 if h else H0)

    z_first = Ring(lambda r, h: p.at[:, q2(r, h)], lambda r, h: p[:, q2(r, h), :],
                   zb0, zb1, zc0, zc1, zp, zm)
    def zh(h):
        return pl.ds(H0 * h, H1 if h else H0)
    z_then = Ring(lambda r, h: zr.at[r, zh(h)], lambda r, h: zr[r, zh(h), :],
                  yb0, yb1, yc0, yc1, yp, ym)
    z_out = Spread(R1, Q2, H0)

    for h in (0, 1):
        late(R1 // 2 * h, R1 // 2, xa)
        y_first.far_half(h)
    for r in (2, 1, 3, 0):
        second_part(r)
    z_first.far()
    z_first.near()
    first_part(1)
    first_part(3)
    y_first.near()

    lt[...] = l[0:704, :].T

    def token_grads(rel):
        rows = jnp.concatenate([lt[slot(k, rel):slot(k, rel) + ROWS, :] for k in range(4)], axis=0)
        return nn(rows, w[0:704, :])

    pb[...] = token_grads(1).astype(BF16)
    pair = send(pb, rb, twin)
    s0[...] = token_grads(0)

    y_first.middle()
    z_first.middle()
    pair.wait_recv()
    sb[...] = (s0[...] + rb[...].astype(F32)).astype(BF16)
    chip = {0: 0, 3: 1, 1: 2, 2: 3}
    def xh(r, h):
        return pl.ds(ROWS * chip[r] + 48 * h, 48)
    x_ring = Ring(lambda r, h: sb.at[xh(r, h)], lambda r, h: sb[xh(r, h), :],
                  xr.at[0], xr.at[1], xs.at[0], xs.at[1], xp, xm)
    x_ring.far()
    x_ring.near()
    first_part(0)
    drain(14)

    zr[:, 0:H0, :] = z_first.end(0)
    zr[:, H0:Q2, :] = z_first.end(1)
    z_then.far()
    z_then.near()
    yr[0:R1 // 2, :] = y_first.end(0)
    swaps[0].start()
    swaps[1].start()
    yr[R1 // 2:R1, :] = y_first.end(1)
    swaps[2].start()
    swaps[3].start()
    drain(8)
    x_ring.middle()
    z_then.middle()
    for h in (0, 1):
        out[z_out_rows(z, h), :] = z_then.end(h)
        z_out.start(h)
    for i in (0, 2, 1, 3):
        swaps[i].middle()
    drain(8)
    gi_ref[0:48, :] = x_ring.end(0)
    gi_ref[48:96, :] = x_ring.end(1)
    z_out.middle()
    for i in (0, 2, 1, 3):
        swaps[i].end()
    z_out.end()
    drain()


def z_out_rows(z, h):
    return pl.ds(pl.multiple_of(R1 + Q2 * z + H0 * h, 16), H1 if h else H0)


def finish(factor, gi_ref, dw_ref, gi_hbm, og_hbm, ou_hbm, od_hbm, gi, og, ou, od, sems):
    copies = []
    for i, (buf, dst) in enumerate(((gi, gi_hbm), (og, og_hbm), (ou, ou_hbm), (od, od_hbm))):
        if i == 0:
            buf[...] = gi_ref[...]
        else:
            buf[...] = dw_ref[HID * (i - 1):HID * i, :].astype(F32) * factor
        copies.append(pltpu.make_async_copy(buf, dst, sems.at[i]))
        copies[-1].start()
    for c in copies:
        c.wait()


def body(tokens_in, out_grad, gate_weight, up_weight, down_weight):
    factor = (ROWS * 128) ** (-0.5)
    vmem = pl.BlockSpec(memory_space=pltpu.VMEM)
    hbm = pl.BlockSpec(memory_space=pl.ANY)
    grad_in, sums = pl.pallas_call(
        kernel,
        name="ffn_backward",
        out_shape=(pltpu.VMEM((ROWS, WIDTH), BF16), pltpu.VMEM((RP, SHARD), BF16)),
        in_specs=[pl.BlockSpec(memory_space=pl.ANY)] * 5,
        out_specs=(vmem, vmem),
        scratch_shapes=[
            pltpu.VMEM((TOK, WIDTH), BF16),
            pltpu.VMEM((TOK, WIDTH), BF16),
            pltpu.VMEM((3 * HID, WIDTH), BF16),
            pltpu.VMEM((3 * HID, TOK), F32),
            pltpu.VMEM((RP, TOK), BF16),
            pltpu.VMEM((TOK, 2 * HID), BF16),
            pltpu.VMEM((R1, SHARD), F32),
            pltpu.VMEM((4, R2, SHARD), F32),
            pltpu.VMEM((4, RP, SHARD), BF16),
            pltpu.VMEM((384, WIDTH), BF16),
            pltpu.VMEM((384, WIDTH), BF16),
            pltpu.VMEM((384, WIDTH), F32),
            pltpu.VMEM((384, WIDTH), BF16),
            pltpu.VMEM((2, 3, 48, WIDTH), BF16),
            pltpu.VMEM((2, 48, WIDTH), BF16),
            pltpu.VMEM((2, 3, R1 // 2, SHARD), BF16),
            pltpu.VMEM((2, R1 // 2, SHARD), BF16),
            pltpu.VMEM((R1, SHARD), BF16),
            pltpu.VMEM((2, R1, SHARD), BF16),
            pltpu.VMEM((R1, SHARD), BF16),
            pltpu.VMEM((3, 4, H0, SHARD), BF16),
            pltpu.VMEM((3, 4, H1, SHARD), BF16),
            pltpu.VMEM((4, H0, SHARD), BF16),
            pltpu.VMEM((4, H1, SHARD), BF16),
            pltpu.VMEM((4, Q2, SHARD), BF16),
            pltpu.VMEM((3, H0, SHARD), BF16),
            pltpu.VMEM((3, H1, SHARD), BF16),
            pltpu.VMEM((H0, SHARD), BF16),
            pltpu.VMEM((H1, SHARD), BF16),
            pltpu.SemaphoreType.DMA((5,)),
            pltpu.SemaphoreType.DMA((96,)),
            pltpu.SemaphoreType.DMA((96,)),
        ],
        compiler_params=pltpu.CompilerParams(collective_id=0, has_side_effects=True),
    )(tokens_in, out_grad, gate_weight.T, up_weight.T, down_weight)
    grad_in, gg, gu, gd = pl.pallas_call(
        functools.partial(finish, factor),
        name="finish",
        out_shape=(jax.ShapeDtypeStruct((ROWS, WIDTH), BF16),) + (jax.ShapeDtypeStruct((HID, SHARD), F32),) * 3,
        in_specs=[vmem, vmem],
        out_specs=(hbm,) * 4,
        scratch_shapes=[pltpu.VMEM((ROWS, WIDTH), BF16)] + [pltpu.VMEM((HID, SHARD), F32)] * 3
        + [pltpu.SemaphoreType.DMA((4,))],
        compiler_params=pltpu.CompilerParams(vmem_limit_bytes=8 << 20),
    )(grad_in, sums)
    return grad_in, gg.T, gu.T, gd


def solution(mesh):
    return jax.shard_map(
        body,
        mesh=mesh,
        in_specs=(
            P(("rep", "fs", "tp"), None),
            P(("rep", "fs", "tp"), None),
            P("fs", "tp"),
            P("fs", "tp"),
            P("tp", "fs"),
        ),
        out_specs=(P(("rep", "fs", "tp"), None), P("fs", "tp"), P("fs", "tp"), P("tp", "fs")),
        check_vma=False,
    )
```

```python
import functools

import jax
import jax.numpy as jnp
from jax import lax
from jax.experimental import pallas as pl
from jax.experimental.pallas import tpu as pltpu
from jax.sharding import PartitionSpec as P

MESH = pl.DeviceIdType.MESH
F32 = jnp.float32
BF16 = jnp.bfloat16

ROWS = 96
WIDTH = 1024
HID = 352
SHARD = 256
TOK = 768
EARLY = 512
R1 = 576
R2 = 512
RP = R1 + R2
PIECE, Q2 = R1 // 4, R2 // 4
H0, H1 = 64, 64


AT = (3, 0, 1, 2)


def nt(a, b):
    return lax.dot_general(a, b, (((1,), (1,)), ((), ())), preferred_element_type=F32)


def nn(a, b):
    return lax.dot_general(a, b, (((1,), (0,)), ((), ())), preferred_element_type=F32)


def aligned(value, by):
    return pl.multiple_of(value, by)


def kernel(x_hbm, o_hbm, g_hbm, u_hbm, d_hbm, gi_ref, out,
           xa, oa, w, fwd, l, lt, pa, pz, p, pb, rb, s0, sb, xr, xs,
           ya, ys, yr, got, half_sum, zb0, zb1, zc0, zc1, zr, yb0, yb1, yc0, yc1,
           ls, ss, rs):
    z = lax.axis_index("rep")
    y = lax.axis_index("fs")
    t = lax.axis_index("tp")
    core = lax.rem(t, 2)
    half = lax.rem(z, 2)
    xp = (z, y, lax.rem(t + 2, 8))
    xm = (z, y, lax.rem(t + 6, 8))
    twin = (z, y, t + 1 - 2 * core)
    yp = (z, lax.rem(y + 1, 4), t)
    ym = (z, lax.rem(y + 3, 4), t)
    zp = (lax.rem(z + 1, 4), y, t)
    zm = (lax.rem(z + 3, 4), y, t)

    counter = [0]
    started = []

    def send(src, dst, dev):
        i = counter[0]
        counter[0] += 1
        copy = pltpu.make_async_remote_copy(
            src_ref=src, dst_ref=dst, send_sem=ss.at[i], recv_sem=rs.at[i],
            device_id=dev, device_id_type=MESH)
        copy.start()
        started.append(copy)
        return copy

    def drain(keep=0):
        while len(started) > keep:
            started.pop(0).wait_send()

    mine = pl.ds(aligned(y * SHARD, SHARD), SHARD)
    locals_ = [
        pltpu.make_async_copy(x_hbm, xa.at[pl.ds(0, ROWS)], ls.at[0]),
        pltpu.make_async_copy(g_hbm, w.at[pl.ds(0, HID), mine], ls.at[1]),
        pltpu.make_async_copy(u_hbm, w.at[pl.ds(HID, HID), mine], ls.at[2]),
        pltpu.make_async_copy(d_hbm, w.at[pl.ds(2 * HID, HID), mine], ls.at[3]),
        pltpu.make_async_copy(o_hbm, oa.at[pl.ds(0, ROWS)], ls.at[4]),
    ]
    for c in locals_:
        c.start()

    barrier = pltpu.get_barrier_semaphore()
    for dev in (xp, xm, twin, yp, ym, zp, zm):
        pl.semaphore_signal(barrier, inc=1, device_id=dev, device_id_type=MESH)
    l[pl.ds(3 * HID, RP - 3 * HID), :] = jnp.zeros((RP - 3 * HID, TOK), BF16)
    pl.semaphore_wait(barrier, 7)

    def slot(k, rel):
        return 2 * ROWS * k + ROWS * rel

    def tok(ref, row, n):
        return ref.at[pl.ds(row, n)]

    my_rows = [aligned(640 * half, 16), aligned(640 * half + 208, 16), 416]

    def wblk(row, n, col):
        return w.at[pl.ds(row, n), pl.ds(aligned(lax.rem(col, 4) * SHARD, SHARD), SHARD)]

    def wsend(i, off, n, col, dev):
        ref = wblk(my_rows[i] + off if off else my_rows[i], n, col)
        return send(ref, ref, dev)

    for c in locals_[:1]:
        c.wait()
    x_p = send(tok(xa, 0, ROWS), tok(xa, slot(1, 0), ROWS), xp)
    x_m = send(tok(xa, 0, ROWS), tok(xa, slot(2, 0), ROWS), xm)
    x_t = send(tok(xa, 0, ROWS), tok(xa, slot(0, 1), ROWS), twin)
    for c in locals_[1:4]:
        c.wait()
    wp_a = wsend(0, 0, 208, y, yp)
    wm_b = wsend(1, 0, 208, y, ym)
    wp_b = wsend(1, 0, 208, y, yp)
    wm_a = wsend(0, 0, 208, y, ym)
    locals_[4].wait()
    o_p = send(tok(oa, 0, ROWS), tok(oa, slot(1, 0), ROWS), xp)
    o_m = send(tok(oa, 0, ROWS), tok(oa, slot(2, 0), ROWS), xm)
    o_t = send(tok(oa, 0, ROWS), tok(oa, slot(0, 1), ROWS), twin)

    z_in = []

    def zsend(i, col, dev):
        z_in.append(wsend(i, 0, 208, col, dev))

    wp_a.wait_recv()
    fp_a = wsend(0, 0, 208, y + 3, yp)
    zsend(0, y + 3, zp)
    wm_b.wait_recv()
    fm_b = wsend(1, 0, 208, y + 1, ym)
    zsend(1, y + 1, zm)
    wp_c = wsend(2, 0, 224, y, yp)
    wm_c = wsend(2, 0, 224, y, ym)

    x_p.wait_recv()
    xf_p = send(tok(xa, slot(1, 0), 48), tok(xa, slot(3, 0), 48), xp)
    x_m.wait_recv()
    xf_m = send(tok(xa, slot(2, 0) + 48, 48), tok(xa, slot(3, 0) + 48, 48), xm)
    xt1 = send(tok(xa, slot(1, 0), ROWS), tok(xa, slot(1, 1), ROWS), twin)
    xt2 = send(tok(xa, slot(2, 0), ROWS), tok(xa, slot(2, 1), ROWS), twin)

    wp_b.wait_recv()
    zsend(1, y + 3, zm)
    wm_a.wait_recv()
    zsend(0, y + 1, zp)
    fp_a.wait_recv()
    zsend(0, y + 2, zp)
    fm_b.wait_recv()
    zsend(1, y + 2, zm)

    wp_c.wait_recv()
    fp_c = wsend(2, 0, 112, y + 3, yp)
    wm_c.wait_recv()
    fm_c = wsend(2, 112, 112, y + 1, ym)

    o_p.wait_recv()
    of_p = send(tok(oa, slot(1, 0), 48), tok(oa, slot(3, 0), 48), xp)
    o_m.wait_recv()
    of_m = send(tok(oa, slot(2, 0) + 48, 48), tok(oa, slot(3, 0) + 48, 48), xm)
    ot1 = send(tok(oa, slot(1, 0), ROWS), tok(oa, slot(1, 1), ROWS), twin)
    ot2 = send(tok(oa, slot(2, 0), ROWS), tok(oa, slot(2, 1), ROWS), twin)

    xf_p.wait_recv()
    xt3 = send(tok(xa, slot(3, 0), 48), tok(xa, slot(3, 1), 48), twin)
    xf_m.wait_recv()
    xt4 = send(tok(xa, slot(3, 0) + 48, 48), tok(xa, slot(3, 1) + 48, 48), twin)
    for c in (fp_c, fm_c):
        c.wait_recv()
    for c in z_in:
        c.wait_recv()
    for c in (x_t, o_t, xt1, xt2, ot1, ot2):
        c.wait_recv()

    def project(c0, n, parts=(0, 1, 2)):
        cols = pl.ds(c0, n)
        for part in parts:
            source = oa if part == 2 else xa
            rows = pl.ds(HID * part, HID)
            fwd[rows, cols] = nt(w[rows, :], source[cols, :])

    def elementwise(c0, n):
        cols = pl.ds(c0, n)
        for m in range(11):
            a = 32 * m
            g = fwd[a:a + 32, cols].astype(BF16).astype(F32)
            u = fwd[HID + a:HID + a + 32, cols].astype(BF16).astype(F32)
            gh = fwd[2 * HID + a:2 * HID + a + 32, cols].astype(BF16).astype(F32)
            sig = 1.0 / (1.0 + jnp.exp(-g))
            act = g * sig
            l[a:a + 32, cols] = (gh * u * sig * (1.0 + g * (1.0 - sig))).astype(BF16)
            l[HID + a:HID + a + 32, cols] = (gh * act).astype(BF16)
            l[2 * HID + a:2 * HID + a + 32, cols] = (act * u).astype(BF16)

    def shard_cols(r):
        return pl.ds(aligned(lax.rem(y + r, 4) * SHARD, SHARD), SHARD)

    def early(row, n, source):
        pa[row:row + n, :] = nn(l[row:row + n, 0:EARLY], source[0:EARLY, shard_cols(2)])

    def late(row, n, source):
        more = nn(l[row:row + n, EARLY:TOK], source[EARLY:TOK, shard_cols(2)])
        p[AT[2], row:row + n, :] = (pa[row:row + n, :] + more).astype(BF16)

    def whole(r, row, n, source):
        p[AT[r], row:row + n, :] = nn(l[row:row + n, :], source[:, shard_cols(r)]).astype(BF16)

    def early_second(r):
        pz[r, 0:704 - R1, :] = nn(l[R1:704, 0:EARLY], xa[0:EARLY, shard_cols(r)])
        pz[r, 704 - R1:R2, :] = nn(l[704:RP, 0:EARLY], oa[0:EARLY, shard_cols(r)])

    def first_part(r):
        whole(r, 0, R1 // 2, xa)
        whole(r, R1 // 2, R1 // 2, xa)

    def second_part(r):
        more = nn(l[R1:704, EARLY:TOK], xa[EARLY:TOK, shard_cols(r)])
        p[AT[r], R1:704, :] = (pz[r, 0:704 - R1, :] + more).astype(BF16)
        more = nn(l[704:RP, EARLY:TOK], oa[EARLY:TOK, shard_cols(r)])
        p[AT[r], 704:RP, :] = (pz[r, 704 - R1:R2, :] + more).astype(BF16)

    project(0, 256)
    elementwise(0, 256)
    of_p.wait_recv()
    ot3 = send(tok(oa, slot(3, 0), 48), tok(oa, slot(3, 1), 48), twin)
    of_m.wait_recv()
    ot4 = send(tok(oa, slot(3, 0) + 48, 48), tok(oa, slot(3, 1) + 48, 48), twin)
    project(256, EARLY - 256)
    elementwise(256, EARLY - 256)
    xt3.wait_recv()
    xt4.wait_recv()
    project(EARLY, TOK - EARLY, (0, 1))
    early(0, R1 // 2, xa)
    early(R1 // 2, R1 // 2, xa)
    for r in (2, 1, 3, 0):
        early_second(r)
    ot3.wait_recv()
    ot4.wait_recv()
    project(EARLY, TOK - EARLY, (2,))
    elementwise(EARLY, TOK - EARLY)

    class Ring:
        def __init__(self, block, load, b0, b1, c0, c1, plus, minus):
            self.block, self.load = block, load
            self.b0, self.b1, self.c0, self.c1 = b0, b1, c0, c1
            self.plus, self.minus = plus, minus

        def far(self):
            self.far_half(0)
            self.far_half(1)

        def far_half(self, h):
            if h:
                self.a1 = send(self.block(2, 1), self.b1.at[0], self.minus)
            else:
                self.a0 = send(self.block(2, 0), self.b0.at[0], self.plus)

        def near(self):
            self.near_half(1)
            self.near_half(0)

        def near_half(self, h):
            if h:
                self.n1 = send(self.block(1, 1), self.b1.at[1], self.plus)
            else:
                self.n0 = send(self.block(3, 0), self.b0.at[1], self.minus)

        def middle(self):
            self.a0.wait_recv()
            self.c0[...] = (self.b0[0].astype(F32) + self.load(1, 0).astype(F32)).astype(BF16)
            self.e0 = send(self.c0, self.b0.at[2], self.plus)
            self.a1.wait_recv()
            self.c1[...] = (self.b1[0].astype(F32) + self.load(3, 1).astype(F32)).astype(BF16)
            self.e1 = send(self.c1, self.b1.at[2], self.minus)

        def end(self, h):
            for c in ((self.n1, self.e1) if h else (self.n0, self.e0)):
                c.wait_recv()
            got = self.b1 if h else self.b0
            return (self.load(0, h).astype(F32) + got[1].astype(F32) + got[2].astype(F32)).astype(BF16)

    class Spread:
        def __init__(self, base, size, cut):
            self.base, self.size, self.cut = base, size, cut

        def rows(self, r, off, n):
            return out.at[pl.ds(aligned(self.base + self.size * lax.rem(z + r, 4) + off, 16), n)]

        def part(self, r, h):
            return self.rows(r, self.cut * h, self.size - self.cut if h else self.cut)

        def start(self, h):
            ref = self.part(0, h)
            if h:
                self.m1 = send(ref, ref, zm)
                self.p1 = send(ref, ref, zp)
            else:
                self.p0 = send(ref, ref, zp)
                self.m0 = send(ref, ref, zm)

        def middle(self):
            self.p0.wait_recv()
            ref = self.part(3, 0)
            self.f0 = send(ref, ref, zp)
            self.m1.wait_recv()
            ref = self.part(1, 1)
            self.f1 = send(ref, ref, zm)

        def end(self):
            for c in (self.m0, self.p1, self.f0, self.f1):
                c.wait_recv()

    def y_ring(k):
        def rows(h):
            return pl.ds(R1 // 2 * h + PIECE * k, PIECE)
        return Ring(lambda r, h: p.at[AT[r], rows(h)], lambda r, h: p[AT[r], rows(h), :],
                    ya.at[k, 0], ya.at[k, 1], ys.at[k, 0], ys.at[k, 1], yp, ym)

    y_first = [y_ring(0), y_ring(1)]

    pair_a = (z + 1 - 2 * half, y, t)
    pair_b = (lax.rem(z + 3 + 2 * half, 4), y, t)

    class Exchange:
        def __init__(self, i):
            self.i, self.rows = i, pl.ds(PIECE * i, PIECE)
            self.first, self.second = (pair_a, pair_b) if i < 2 else (pair_b, pair_a)

        def start(self):
            self.c0 = send(yr.at[self.rows], got.at[0, self.rows], self.first)

        def middle(self):
            self.c0.wait_recv()
            half_sum[self.rows, :] = (yr[self.rows, :].astype(F32) + got[0, self.rows, :].astype(F32)).astype(BF16)
            self.c1 = send(half_sum.at[self.rows], got.at[1, self.rows], self.second)

        def end(self):
            self.c1.wait_recv()
            out[self.rows, :] = (half_sum[self.rows, :].astype(F32) + got[1, self.rows, :].astype(F32)).astype(BF16)

    swaps = [Exchange(i) for i in range(4)]

    def q2(r, h):
        return pl.ds(aligned(R1 + Q2 * lax.rem(z + r, 4) + H0 * h, 16), H1 if h else H0)

    def z_ring(k):
        two = pl.ds(2 * k, 2)
        return Ring(lambda r, h: p.at[two, q2(r, h)], lambda r, h: p[two, q2(r, h), :],
                    zb0.at[k], zb1.at[k], zc0.at[k], zc1.at[k], zp, zm)

    z_first = [z_ring(0), z_ring(1)]

    def zh(h):
        return pl.ds(H0 * h, H1 if h else H0)
    z_then = Ring(lambda r, h: zr.at[AT[r], zh(h)], lambda r, h: zr[AT[r], zh(h), :],
                  yb0, yb1, yc0, yc1, yp, ym)
    z_out = Spread(R1, Q2, H0)

    for h in (0, 1):
        late(R1 // 2 * h, R1 // 2, xa)
        y_first[0].far_half(h)
        y_first[1].far_half(h)
    for r in (2, 1, 3, 0):
        second_part(r)
    z_first[0].far()
    z_first[1].far()
    z_first[0].near()
    z_first[1].near()
    first_part(1)
    first_part(3)
    y_first[0].near()
    y_first[1].near()

    lt[...] = l[0:704, :].T

    def token_grads(rel):
        rows = jnp.concatenate([lt[slot(k, rel):slot(k, rel) + ROWS, :] for k in range(4)], axis=0)
        return nn(rows, w[0:704, :])

    pb[...] = token_grads(1).astype(BF16)
    pair = send(pb, rb, twin)
    s0[...] = token_grads(0)

    y_first[0].middle()
    z_first[0].middle()
    y_first[1].middle()
    z_first[1].middle()
    pair.wait_recv()
    sb[...] = (s0[...] + rb[...].astype(F32)).astype(BF16)
    chip = {0: 0, 3: 1, 1: 2, 2: 3}
    def xh(r, h):
        return pl.ds(ROWS * chip[r] + 48 * h, 48)
    x_ring = Ring(lambda r, h: sb.at[xh(r, h)], lambda r, h: sb[xh(r, h), :],
                  xr.at[0], xr.at[1], xs.at[0], xs.at[1], xp, xm)
    x_ring.far()
    x_ring.near()
    first_part(0)
    drain(16)

    for h in (0, 1):
        zr[0:2, zh(h), :] = z_first[0].end(h)
    z_then.far()
    z_then.near_half(1)
    for k in (0, 1):
        for h in (0, 1):
            yr[pl.ds(R1 // 2 * h + PIECE * k, PIECE), :] = y_first[k].end(h)
            swaps[2 * h + k].start()
        if k == 0:
            for h in (0, 1):
                zr[2:4, zh(h), :] = z_first[1].end(h)
            z_then.near_half(0)
    drain(8)
    x_ring.middle()
    z_then.middle()
    for h in (0, 1):
        out[z_out_rows(z, h), :] = z_then.end(h)
        z_out.start(h)
    for i in (0, 2, 1, 3):
        swaps[i].middle()
    drain(8)
    gi_ref[0:48, :] = x_ring.end(0)
    gi_ref[48:96, :] = x_ring.end(1)
    z_out.middle()
    for i in (0, 2, 1, 3):
        swaps[i].end()
    z_out.end()
    drain()


def z_out_rows(z, h):
    return pl.ds(pl.multiple_of(R1 + Q2 * z + H0 * h, 16), H1 if h else H0)


def finish(factor, gi_ref, dw_ref, gi_hbm, og_hbm, ou_hbm, od_hbm, gi, og, ou, od, sems):
    copies = []
    for i, (buf, dst) in enumerate(((gi, gi_hbm), (og, og_hbm), (ou, ou_hbm), (od, od_hbm))):
        if i == 0:
            buf[...] = gi_ref[...]
        else:
            buf[...] = dw_ref[HID * (i - 1):HID * i, :].astype(F32) * factor
        copies.append(pltpu.make_async_copy(buf, dst, sems.at[i]))
        copies[-1].start()
    for c in copies:
        c.wait()


def body(tokens_in, out_grad, gate_weight, up_weight, down_weight):
    factor = (ROWS * 128) ** (-0.5)
    vmem = pl.BlockSpec(memory_space=pltpu.VMEM)
    hbm = pl.BlockSpec(memory_space=pl.ANY)
    grad_in, sums = pl.pallas_call(
        kernel,
        name="ffn_backward",
        out_shape=(pltpu.VMEM((ROWS, WIDTH), BF16), pltpu.VMEM((RP, SHARD), BF16)),
        in_specs=[pl.BlockSpec(memory_space=pl.ANY)] * 5,
        out_specs=(vmem, vmem),
        scratch_shapes=[
            pltpu.VMEM((TOK, WIDTH), BF16),
            pltpu.VMEM((TOK, WIDTH), BF16),
            pltpu.VMEM((3 * HID, WIDTH), BF16),
            pltpu.VMEM((3 * HID, TOK), F32),
            pltpu.VMEM((RP, TOK), BF16),
            pltpu.VMEM((TOK, 2 * HID), BF16),
            pltpu.VMEM((R1, SHARD), F32),
            pltpu.VMEM((4, R2, SHARD), F32),
            pltpu.VMEM((4, RP, SHARD), BF16),
            pltpu.VMEM((384, WIDTH), BF16),
            pltpu.VMEM((384, WIDTH), BF16),
            pltpu.VMEM((384, WIDTH), F32),
            pltpu.VMEM((384, WIDTH), BF16),
            pltpu.VMEM((2, 3, 48, WIDTH), BF16),
            pltpu.VMEM((2, 48, WIDTH), BF16),
            pltpu.VMEM((2, 2, 3, PIECE, SHARD), BF16),
            pltpu.VMEM((2, 2, PIECE, SHARD), BF16),
            pltpu.VMEM((R1, SHARD), BF16),
            pltpu.VMEM((2, R1, SHARD), BF16),
            pltpu.VMEM((R1, SHARD), BF16),
            pltpu.VMEM((2, 3, 2, H0, SHARD), BF16),
            pltpu.VMEM((2, 3, 2, H1, SHARD), BF16),
            pltpu.VMEM((2, 2, H0, SHARD), BF16),
            pltpu.VMEM((2, 2, H1, SHARD), BF16),
            pltpu.VMEM((4, Q2, SHARD), BF16),
            pltpu.VMEM((3, H0, SHARD), BF16),
            pltpu.VMEM((3, H1, SHARD), BF16),
            pltpu.VMEM((H0, SHARD), BF16),
            pltpu.VMEM((H1, SHARD), BF16),
            pltpu.SemaphoreType.DMA((5,)),
            pltpu.SemaphoreType.DMA((112,)),
            pltpu.SemaphoreType.DMA((112,)),
        ],
        compiler_params=pltpu.CompilerParams(collective_id=0, has_side_effects=True),
    )(tokens_in, out_grad, gate_weight.T, up_weight.T, down_weight)
    grad_in, gg, gu, gd = pl.pallas_call(
        functools.partial(finish, factor),
        name="finish",
        out_shape=(jax.ShapeDtypeStruct((ROWS, WIDTH), BF16),) + (jax.ShapeDtypeStruct((HID, SHARD), F32),) * 3,
        in_specs=[vmem, vmem],
        out_specs=(hbm,) * 4,
        scratch_shapes=[pltpu.VMEM((ROWS, WIDTH), BF16)] + [pltpu.VMEM((HID, SHARD), F32)] * 3
        + [pltpu.SemaphoreType.DMA((4,))],
        compiler_params=pltpu.CompilerParams(vmem_limit_bytes=8 << 20),
    )(grad_in, sums)
    return grad_in, gg.T, gu.T, gd


def solution(mesh):
    return jax.shard_map(
        body,
        mesh=mesh,
        in_specs=(
            P(("rep", "fs", "tp"), None),
            P(("rep", "fs", "tp"), None),
            P("fs", "tp"),
            P("fs", "tp"),
            P("tp", "fs"),
        ),
        out_specs=(P(("rep", "fs", "tp"), None), P("fs", "tp"), P("fs", "tp"), P("tp", "fs")),
        check_vma=False,
    )
```

```python
import functools

import jax
import jax.numpy as jnp
from jax import lax
from jax.experimental import pallas as pl
from jax.experimental.pallas import tpu as pltpu
from jax.sharding import PartitionSpec as P

MESH = pl.DeviceIdType.MESH
F32 = jnp.float32
BF16 = jnp.bfloat16

ROWS = 96
WIDTH = 1024
HID = 352
SHARD = 256
TOK = 768
EARLY = 512
R1 = 576
R2 = 512
RP = R1 + R2
PIECE, Q2 = R1 // 4, R2 // 4
H0, H1 = 64, 64


AT = (3, 0, 1, 2)


def nt(a, b):
    return lax.dot_general(a, b, (((1,), (1,)), ((), ())), preferred_element_type=F32)


def nn(a, b):
    return lax.dot_general(a, b, (((1,), (0,)), ((), ())), preferred_element_type=F32)


def aligned(value, by):
    return pl.multiple_of(value, by)


def kernel(x_hbm, o_hbm, g_hbm, u_hbm, d_hbm, gi_ref, out,
           xa, oa, w, fwd, l, lt, pa, pz, p, pb, rb, s0, sb, xr, xs,
           ya, ys, yr, got, half_sum, zb0, zb1, zc0, zc1, zr, yb0, yb1, yc0, yc1,
           ls, ss, rs):
    z = lax.axis_index("rep")
    y = lax.axis_index("fs")
    t = lax.axis_index("tp")
    core = lax.rem(t, 2)
    half = lax.rem(z, 2)
    xp = (z, y, lax.rem(t + 2, 8))
    xm = (z, y, lax.rem(t + 6, 8))
    twin = (z, y, t + 1 - 2 * core)
    yp = (z, lax.rem(y + 1, 4), t)
    ym = (z, lax.rem(y + 3, 4), t)
    zp = (lax.rem(z + 1, 4), y, t)
    zm = (lax.rem(z + 3, 4), y, t)

    counter = [0]
    started = []

    def send(src, dst, dev):
        i = counter[0]
        counter[0] += 1
        copy = pltpu.make_async_remote_copy(
            src_ref=src, dst_ref=dst, send_sem=ss.at[i], recv_sem=rs.at[i],
            device_id=dev, device_id_type=MESH)
        copy.start()
        started.append(copy)
        return copy

    def drain(keep=0):
        while len(started) > keep:
            started.pop(0).wait_send()

    mine = pl.ds(aligned(y * SHARD, SHARD), SHARD)
    locals_ = [
        pltpu.make_async_copy(x_hbm, xa.at[pl.ds(0, ROWS)], ls.at[0]),
        pltpu.make_async_copy(g_hbm, w.at[pl.ds(0, HID), mine], ls.at[1]),
        pltpu.make_async_copy(u_hbm, w.at[pl.ds(HID, HID), mine], ls.at[2]),
        pltpu.make_async_copy(d_hbm, w.at[pl.ds(2 * HID, HID), mine], ls.at[3]),
        pltpu.make_async_copy(o_hbm, oa.at[pl.ds(0, ROWS)], ls.at[4]),
    ]
    for c in locals_:
        c.start()

    barrier = pltpu.get_barrier_semaphore()
    for dev in (xp, xm, twin, yp, ym, zp, zm):
        pl.semaphore_signal(barrier, inc=1, device_id=dev, device_id_type=MESH)
    l[pl.ds(3 * HID, RP - 3 * HID), :] = jnp.zeros((RP - 3 * HID, TOK), BF16)
    pl.semaphore_wait(barrier, 7)

    def slot(k, rel):
        return 2 * ROWS * k + ROWS * rel

    def tok(ref, row, n):
        return ref.at[pl.ds(row, n)]

    my_rows = [aligned(640 * half, 16), aligned(640 * half + 208, 16), 416]

    def wblk(row, n, col):
        return w.at[pl.ds(row, n), pl.ds(aligned(lax.rem(col, 4) * SHARD, SHARD), SHARD)]

    def wsend(i, off, n, col, dev):
        ref = wblk(my_rows[i] + off if off else my_rows[i], n, col)
        return send(ref, ref, dev)

    for c in locals_[:1]:
        c.wait()
    x_p = send(tok(xa, 0, ROWS), tok(xa, slot(1, 0), ROWS), xp)
    x_m = send(tok(xa, 0, ROWS), tok(xa, slot(2, 0), ROWS), xm)
    x_t = send(tok(xa, 0, ROWS), tok(xa, slot(0, 1), ROWS), twin)
    for c in locals_[1:4]:
        c.wait()
    wp_a = wsend(0, 0, 208, y, yp)
    wm_b = wsend(1, 0, 208, y, ym)
    wp_b = wsend(1, 0, 208, y, yp)
    wm_a = wsend(0, 0, 208, y, ym)
    locals_[4].wait()
    o_p = send(tok(oa, 0, ROWS), tok(oa, slot(1, 0), ROWS), xp)
    o_m = send(tok(oa, 0, ROWS), tok(oa, slot(2, 0), ROWS), xm)
    o_t = send(tok(oa, 0, ROWS), tok(oa, slot(0, 1), ROWS), twin)

    z_in = []

    def zsend(i, col, dev):
        z_in.append(wsend(i, 0, 208, col, dev))

    wp_a.wait_recv()
    fp_a = wsend(0, 0, 208, y + 3, yp)
    zsend(0, y + 3, zp)
    wm_b.wait_recv()
    fm_b = wsend(1, 0, 208, y + 1, ym)
    zsend(1, y + 1, zm)
    wp_c = wsend(2, 0, 224, y, yp)
    wm_c = wsend(2, 0, 224, y, ym)

    x_p.wait_recv()
    xf_p = send(tok(xa, slot(1, 0), 48), tok(xa, slot(3, 0), 48), xp)
    x_m.wait_recv()
    xf_m = send(tok(xa, slot(2, 0) + 48, 48), tok(xa, slot(3, 0) + 48, 48), xm)
    xt1 = send(tok(xa, slot(1, 0), ROWS), tok(xa, slot(1, 1), ROWS), twin)
    xt2 = send(tok(xa, slot(2, 0), ROWS), tok(xa, slot(2, 1), ROWS), twin)

    wp_b.wait_recv()
    zsend(1, y + 3, zm)
    wm_a.wait_recv()
    zsend(0, y + 1, zp)
    fp_a.wait_recv()
    zsend(0, y + 2, zp)
    fm_b.wait_recv()
    zsend(1, y + 2, zm)

    wp_c.wait_recv()
    fp_c = wsend(2, 0, 112, y + 3, yp)
    wm_c.wait_recv()
    fm_c = wsend(2, 112, 112, y + 1, ym)

    o_p.wait_recv()
    of_p = send(tok(oa, slot(1, 0), 48), tok(oa, slot(3, 0), 48), xp)
    o_m.wait_recv()
    of_m = send(tok(oa, slot(2, 0) + 48, 48), tok(oa, slot(3, 0) + 48, 48), xm)
    ot1 = send(tok(oa, slot(1, 0), ROWS), tok(oa, slot(1, 1), ROWS), twin)
    ot2 = send(tok(oa, slot(2, 0), ROWS), tok(oa, slot(2, 1), ROWS), twin)

    xf_p.wait_recv()
    xt3 = send(tok(xa, slot(3, 0), 48), tok(xa, slot(3, 1), 48), twin)
    xf_m.wait_recv()
    xt4 = send(tok(xa, slot(3, 0) + 48, 48), tok(xa, slot(3, 1) + 48, 48), twin)
    for c in (fp_c, fm_c):
        c.wait_recv()
    for c in z_in:
        c.wait_recv()
    for c in (x_t, o_t, xt1, xt2, ot1, ot2):
        c.wait_recv()

    def project(c0, n, parts=(0, 1, 2)):
        cols = pl.ds(c0, n)
        for part in parts:
            source = oa if part == 2 else xa
            for m in (0, 1):
                rows = pl.ds(HID * part + HID // 2 * m, HID // 2)
                fwd[rows, cols] = nt(w[rows, :], source[cols, :])

    def elementwise(c0, n):
        cols = pl.ds(c0, n)
        for m in range(11):
            a = 32 * m
            g = fwd[a:a + 32, cols].astype(BF16).astype(F32)
            u = fwd[HID + a:HID + a + 32, cols].astype(BF16).astype(F32)
            gh = fwd[2 * HID + a:2 * HID + a + 32, cols].astype(BF16).astype(F32)
            sig = 1.0 / (1.0 + jnp.exp(-g))
            act = g * sig
            l[a:a + 32, cols] = (gh * u * sig * (1.0 + g * (1.0 - sig))).astype(BF16)
            l[HID + a:HID + a + 32, cols] = (gh * act).astype(BF16)
            l[2 * HID + a:2 * HID + a + 32, cols] = (act * u).astype(BF16)

    def shard_cols(r):
        return pl.ds(aligned(lax.rem(y + r, 4) * SHARD, SHARD), SHARD)

    def early(row, n, source):
        pa[row:row + n, :] = nn(l[row:row + n, 0:EARLY], source[0:EARLY, shard_cols(2)])

    def late(row, n, source):
        more = nn(l[row:row + n, EARLY:TOK], source[EARLY:TOK, shard_cols(2)])
        p[AT[2], row:row + n, :] = (pa[row:row + n, :] + more).astype(BF16)

    def whole(r, row, n, source):
        p[AT[r], row:row + n, :] = nn(l[row:row + n, :], source[:, shard_cols(r)]).astype(BF16)

    def early_second(r):
        pz[r, 0:704 - R1, :] = nn(l[R1:704, 0:EARLY], xa[0:EARLY, shard_cols(r)])
        pz[r, 704 - R1:R2, :] = nn(l[704:RP, 0:EARLY], oa[0:EARLY, shard_cols(r)])

    def first_part(r):
        whole(r, 0, R1 // 2, xa)
        whole(r, R1 // 2, R1 // 2, xa)

    def second_part(r):
        more = nn(l[R1:704, EARLY:TOK], xa[EARLY:TOK, shard_cols(r)])
        p[AT[r], R1:704, :] = (pz[r, 0:704 - R1, :] + more).astype(BF16)
        more = nn(l[704:RP, EARLY:TOK], oa[EARLY:TOK, shard_cols(r)])
        p[AT[r], 704:RP, :] = (pz[r, 704 - R1:R2, :] + more).astype(BF16)

    project(0, 256)
    elementwise(0, 256)
    of_p.wait_recv()
    ot3 = send(tok(oa, slot(3, 0), 48), tok(oa, slot(3, 1), 48), twin)
    of_m.wait_recv()
    ot4 = send(tok(oa, slot(3, 0) + 48, 48), tok(oa, slot(3, 1) + 48, 48), twin)
    project(256, EARLY - 256)
    elementwise(256, EARLY - 256)
    xt3.wait_recv()
    xt4.wait_recv()
    project(EARLY, TOK - EARLY, (0, 1))
    early(0, R1 // 2, xa)
    early(R1 // 2, R1 // 2, xa)
    for r in (2, 1, 3, 0):
        early_second(r)
    ot3.wait_recv()
    ot4.wait_recv()
    project(EARLY, TOK - EARLY, (2,))
    elementwise(EARLY, TOK - EARLY)

    class Ring:
        def __init__(self, block, load, b0, b1, c0, c1, plus, minus):
            self.block, self.load = block, load
            self.b0, self.b1, self.c0, self.c1 = b0, b1, c0, c1
            self.plus, self.minus = plus, minus

        def far(self):
            self.far_half(0)
            self.far_half(1)

        def far_half(self, h):
            if h:
                self.a1 = send(self.block(2, 1), self.b1.at[0], self.minus)
            else:
                self.a0 = send(self.block(2, 0), self.b0.at[0], self.plus)

        def near(self):
            self.near_half(1)
            self.near_half(0)

        def near_half(self, h):
            if h:
                self.n1 = send(self.block(1, 1), self.b1.at[1], self.plus)
            else:
                self.n0 = send(self.block(3, 0), self.b0.at[1], self.minus)

        def middle(self):
            self.a0.wait_recv()
            self.c0[...] = (self.b0[0].astype(F32) + self.load(1, 0).astype(F32)).astype(BF16)
            self.e0 = send(self.c0, self.b0.at[2], self.plus)
            self.a1.wait_recv()
            self.c1[...] = (self.b1[0].astype(F32) + self.load(3, 1).astype(F32)).astype(BF16)
            self.e1 = send(self.c1, self.b1.at[2], self.minus)

        def end(self, h):
            for c in ((self.n1, self.e1) if h else (self.n0, self.e0)):
                c.wait_recv()
            got = self.b1 if h else self.b0
            return (self.load(0, h).astype(F32) + got[1].astype(F32) + got[2].astype(F32)).astype(BF16)

    class Spread:
        def __init__(self, base, size, cut):
            self.base, self.size, self.cut = base, size, cut

        def rows(self, r, off, n):
            return out.at[pl.ds(aligned(self.base + self.size * lax.rem(z + r, 4) + off, 16), n)]

        def part(self, r, h):
            return self.rows(r, self.cut * h, self.size - self.cut if h else self.cut)

        def start(self, h):
            ref = self.part(0, h)
            if h:
                self.m1 = send(ref, ref, zm)
                self.p1 = send(ref, ref, zp)
            else:
                self.p0 = send(ref, ref, zp)
                self.m0 = send(ref, ref, zm)

        def middle(self):
            self.p0.wait_recv()
            ref = self.part(3, 0)
            self.f0 = send(ref, ref, zp)
            self.m1.wait_recv()
            ref = self.part(1, 1)
            self.f1 = send(ref, ref, zm)

        def end(self):
            for c in (self.m0, self.p1, self.f0, self.f1):
                c.wait_recv()

    def y_ring(k):
        def rows(h):
            return pl.ds(R1 // 2 * h + PIECE * k, PIECE)
        return Ring(lambda r, h: p.at[AT[r], rows(h)], lambda r, h: p[AT[r], rows(h), :],
                    ya.at[k, 0], ya.at[k, 1], ys.at[k, 0], ys.at[k, 1], yp, ym)

    y_first = [y_ring(0), y_ring(1)]

    pair_a = (z + 1 - 2 * half, y, t)
    pair_b = (lax.rem(z + 3 + 2 * half, 4), y, t)

    class Exchange:
        def __init__(self, i):
            self.i, self.rows = i, pl.ds(PIECE * i, PIECE)
            self.first, self.second = (pair_a, pair_b) if i < 2 else (pair_b, pair_a)

        def start(self):
            self.c0 = send(yr.at[self.rows], got.at[0, self.rows], self.first)

        def middle(self):
            self.c0.wait_recv()
            half_sum[self.rows, :] = (yr[self.rows, :].astype(F32) + got[0, self.rows, :].astype(F32)).astype(BF16)
            self.c1 = send(half_sum.at[self.rows], got.at[1, self.rows], self.second)

        def end(self):
            self.c1.wait_recv()
            out[self.rows, :] = (half_sum[self.rows, :].astype(F32) + got[1, self.rows, :].astype(F32)).astype(BF16)

    swaps = [Exchange(i) for i in range(4)]

    def q2(r, h):
        return pl.ds(aligned(R1 + Q2 * lax.rem(z + r, 4) + H0 * h, 16), H1 if h else H0)

    def z_ring(k):
        two = pl.ds(2 * k, 2)
        return Ring(lambda r, h: p.at[two, q2(r, h)], lambda r, h: p[two, q2(r, h), :],
                    zb0.at[k], zb1.at[k], zc0.at[k], zc1.at[k], zp, zm)

    z_first = [z_ring(0), z_ring(1)]

    def zh(h):
        return pl.ds(H0 * h, H1 if h else H0)
    z_then = Ring(lambda r, h: zr.at[AT[r], zh(h)], lambda r, h: zr[AT[r], zh(h), :],
                  yb0, yb1, yc0, yc1, yp, ym)
    z_out = Spread(R1, Q2, H0)

    for h in (0, 1):
        late(R1 // 2 * h, R1 // 2, xa)
        y_first[0].far_half(h)
        y_first[1].far_half(h)
    for r in (2, 1, 3, 0):
        second_part(r)
    z_first[0].far()
    z_first[1].far()
    z_first[0].near()
    z_first[1].near()
    first_part(1)
    first_part(3)
    y_first[0].near()
    y_first[1].near()

    lt[...] = l[0:704, :].T

    def token_grads(rel):
        rows = jnp.concatenate([lt[slot(k, rel):slot(k, rel) + ROWS, :] for k in range(4)], axis=0)
        return nn(rows, w[0:704, :])

    pb[...] = token_grads(1).astype(BF16)
    pair = send(pb, rb, twin)
    s0[...] = token_grads(0)

    y_first[0].middle()
    z_first[0].middle()
    y_first[1].middle()
    z_first[1].middle()
    pair.wait_recv()
    sb[...] = (s0[...] + rb[...].astype(F32)).astype(BF16)
    chip = {0: 0, 3: 1, 1: 2, 2: 3}
    def xh(r, h):
        return pl.ds(ROWS * chip[r] + 48 * h, 48)
    x_ring = Ring(lambda r, h: sb.at[xh(r, h)], lambda r, h: sb[xh(r, h), :],
                  xr.at[0], xr.at[1], xs.at[0], xs.at[1], xp, xm)
    x_ring.far()
    x_ring.near()
    first_part(0)
    drain(16)

    for h in (0, 1):
        zr[0:2, zh(h), :] = z_first[0].end(h)
    z_then.far()
    z_then.near_half(1)
    for k in (0, 1):
        for h in (0, 1):
            yr[pl.ds(R1 // 2 * h + PIECE * k, PIECE), :] = y_first[k].end(h)
            swaps[2 * h + k].start()
        if k == 0:
            for h in (0, 1):
                zr[2:4, zh(h), :] = z_first[1].end(h)
            z_then.near_half(0)
    drain(8)
    x_ring.middle()
    z_then.middle()
    for h in (0, 1):
        out[z_out_rows(z, h), :] = z_then.end(h)
        z_out.start(h)
    for i in (0, 2, 1, 3):
        swaps[i].middle()
    drain(8)
    gi_ref[0:48, :] = x_ring.end(0)
    gi_ref[48:96, :] = x_ring.end(1)
    z_out.middle()
    for i in (0, 2, 1, 3):
        swaps[i].end()
    z_out.end()
    drain()


def z_out_rows(z, h):
    return pl.ds(pl.multiple_of(R1 + Q2 * z + H0 * h, 16), H1 if h else H0)


def finish(factor, gi_ref, dw_ref, gi_hbm, og_hbm, ou_hbm, od_hbm, gi, og, ou, od, sems):
    copies = []
    for i, (buf, dst) in enumerate(((gi, gi_hbm), (og, og_hbm), (ou, ou_hbm), (od, od_hbm))):
        if i == 0:
            buf[...] = gi_ref[...]
        else:
            buf[...] = dw_ref[HID * (i - 1):HID * i, :].astype(F32) * factor
        copies.append(pltpu.make_async_copy(buf, dst, sems.at[i]))
        copies[-1].start()
    for c in copies:
        c.wait()


def body(tokens_in, out_grad, gate_weight, up_weight, down_weight):
    factor = (ROWS * 128) ** (-0.5)
    vmem = pl.BlockSpec(memory_space=pltpu.VMEM)
    hbm = pl.BlockSpec(memory_space=pl.ANY)
    grad_in, sums = pl.pallas_call(
        kernel,
        name="ffn_backward",
        out_shape=(pltpu.VMEM((ROWS, WIDTH), BF16), pltpu.VMEM((RP, SHARD), BF16)),
        in_specs=[pl.BlockSpec(memory_space=pl.ANY)] * 5,
        out_specs=(vmem, vmem),
        scratch_shapes=[
            pltpu.VMEM((TOK, WIDTH), BF16),
            pltpu.VMEM((TOK, WIDTH), BF16),
            pltpu.VMEM((3 * HID, WIDTH), BF16),
            pltpu.VMEM((3 * HID, TOK), F32),
            pltpu.VMEM((RP, TOK), BF16),
            pltpu.VMEM((TOK, 2 * HID), BF16),
            pltpu.VMEM((R1, SHARD), F32),
            pltpu.VMEM((4, R2, SHARD), F32),
            pltpu.VMEM((4, RP, SHARD), BF16),
            pltpu.VMEM((384, WIDTH), BF16),
            pltpu.VMEM((384, WIDTH), BF16),
            pltpu.VMEM((384, WIDTH), F32),
            pltpu.VMEM((384, WIDTH), BF16),
            pltpu.VMEM((2, 3, 48, WIDTH), BF16),
            pltpu.VMEM((2, 48, WIDTH), BF16),
            pltpu.VMEM((2, 2, 3, PIECE, SHARD), BF16),
            pltpu.VMEM((2, 2, PIECE, SHARD), BF16),
            pltpu.VMEM((R1, SHARD), BF16),
            pltpu.VMEM((2, R1, SHARD), BF16),
            pltpu.VMEM((R1, SHARD), BF16),
            pltpu.VMEM((2, 3, 2, H0, SHARD), BF16),
            pltpu.VMEM((2, 3, 2, H1, SHARD), BF16),
            pltpu.VMEM((2, 2, H0, SHARD), BF16),
            pltpu.VMEM((2, 2, H1, SHARD), BF16),
            pltpu.VMEM((4, Q2, SHARD), BF16),
            pltpu.VMEM((3, H0, SHARD), BF16),
            pltpu.VMEM((3, H1, SHARD), BF16),
            pltpu.VMEM((H0, SHARD), BF16),
            pltpu.VMEM((H1, SHARD), BF16),
            pltpu.SemaphoreType.DMA((5,)),
            pltpu.SemaphoreType.DMA((112,)),
            pltpu.SemaphoreType.DMA((112,)),
        ],
        compiler_params=pltpu.CompilerParams(collective_id=0, has_side_effects=True),
    )(tokens_in, out_grad, gate_weight.T, up_weight.T, down_weight)
    grad_in, gg, gu, gd = pl.pallas_call(
        functools.partial(finish, factor),
        name="finish",
        out_shape=(jax.ShapeDtypeStruct((ROWS, WIDTH), BF16),) + (jax.ShapeDtypeStruct((HID, SHARD), F32),) * 3,
        in_specs=[vmem, vmem],
        out_specs=(hbm,) * 4,
        scratch_shapes=[pltpu.VMEM((ROWS, WIDTH), BF16)] + [pltpu.VMEM((HID, SHARD), F32)] * 3
        + [pltpu.SemaphoreType.DMA((4,))],
        compiler_params=pltpu.CompilerParams(vmem_limit_bytes=8 << 20),
    )(grad_in, sums)
    return grad_in, gg.T, gu.T, gd


def solution(mesh):
    return jax.shard_map(
        body,
        mesh=mesh,
        in_specs=(
            P(("rep", "fs", "tp"), None),
            P(("rep", "fs", "tp"), None),
            P("fs", "tp"),
            P("fs", "tp"),
            P("tp", "fs"),
        ),
        out_specs=(P(("rep", "fs", "tp"), None), P("fs", "tp"), P("fs", "tp"), P("tp", "fs")),
        check_vma=False,
    )
```

```python
import functools

import jax
import jax.numpy as jnp
from jax import lax
from jax.experimental import pallas as pl
from jax.experimental.pallas import tpu as pltpu
from jax.sharding import PartitionSpec as P

MESH = pl.DeviceIdType.MESH
F32 = jnp.float32
BF16 = jnp.bfloat16

ROWS = 96
WIDTH = 1024
HID = 352
SHARD = 256
TOK = 768
EARLY = 512
R1 = 576
R2 = 512
RP = R1 + R2
PIECE, Q2 = R1 // 4, R2 // 4
H0, H1 = 64, 64


AT = (3, 0, 1, 2)


def nt(a, b):
    return lax.dot_general(a, b, (((1,), (1,)), ((), ())), preferred_element_type=F32)


def nn(a, b):
    return lax.dot_general(a, b, (((1,), (0,)), ((), ())), preferred_element_type=F32)


def aligned(value, by):
    return pl.multiple_of(value, by)


def kernel(x_hbm, o_hbm, g_hbm, u_hbm, d_hbm, gi_ref, out,
           xa, oa, w, fwd, l, lt, pa, pz, p, pb, rb, s0, sb, xr, xs,
           ya, ys, yr, got, half_sum, zb0, zb1, zc0, zc1, zr, yb0, yb1, yc0, yc1,
           ls, ss, rs):
    z = lax.axis_index("rep")
    y = lax.axis_index("fs")
    t = lax.axis_index("tp")
    core = lax.rem(t, 2)
    half = lax.rem(z, 2)
    xp = (z, y, lax.rem(t + 2, 8))
    xm = (z, y, lax.rem(t + 6, 8))
    twin = (z, y, t + 1 - 2 * core)
    yp = (z, lax.rem(y + 1, 4), t)
    ym = (z, lax.rem(y + 3, 4), t)
    zp = (lax.rem(z + 1, 4), y, t)
    zm = (lax.rem(z + 3, 4), y, t)

    counter = [0]
    started = []

    def send(src, dst, dev):
        i = counter[0]
        counter[0] += 1
        copy = pltpu.make_async_remote_copy(
            src_ref=src, dst_ref=dst, send_sem=ss.at[i], recv_sem=rs.at[i],
            device_id=dev, device_id_type=MESH)
        copy.start()
        started.append(copy)
        return copy

    def drain(keep=0):
        while len(started) > keep:
            started.pop(0).wait_send()

    mine = pl.ds(aligned(y * SHARD, SHARD), SHARD)
    locals_ = [
        pltpu.make_async_copy(x_hbm, xa.at[pl.ds(0, ROWS)], ls.at[0]),
        pltpu.make_async_copy(g_hbm, w.at[pl.ds(0, HID), mine], ls.at[1]),
        pltpu.make_async_copy(u_hbm, w.at[pl.ds(HID, HID), mine], ls.at[2]),
        pltpu.make_async_copy(d_hbm, w.at[pl.ds(2 * HID, HID), mine], ls.at[3]),
        pltpu.make_async_copy(o_hbm, oa.at[pl.ds(0, ROWS)], ls.at[4]),
    ]
    for c in locals_:
        c.start()

    barrier = pltpu.get_barrier_semaphore()
    for dev in (xp, xm, twin, yp, ym, zp, zm):
        pl.semaphore_signal(barrier, inc=1, device_id=dev, device_id_type=MESH)
    l[pl.ds(3 * HID, RP - 3 * HID), :] = jnp.zeros((RP - 3 * HID, TOK), BF16)
    pl.semaphore_wait(barrier, 7)

    def slot(k, rel):
        return 2 * ROWS * k + ROWS * rel

    def tok(ref, row, n):
        return ref.at[pl.ds(row, n)]

    my_rows = [aligned(608 * half, 16), aligned(608 * half + 224, 16), 448]

    def wblk(row, n, col):
        return w.at[pl.ds(row, n), pl.ds(aligned(lax.rem(col, 4) * SHARD, SHARD), SHARD)]

    def wsend(i, off, n, col, dev):
        ref = wblk(my_rows[i] + off if off else my_rows[i], n, col)
        return send(ref, ref, dev)

    for c in locals_[:1]:
        c.wait()
    x_p = send(tok(xa, 0, ROWS), tok(xa, slot(1, 0), ROWS), xp)
    x_m = send(tok(xa, 0, ROWS), tok(xa, slot(2, 0), ROWS), xm)
    x_t = send(tok(xa, 0, ROWS), tok(xa, slot(0, 1), ROWS), twin)
    for c in locals_[1:4]:
        c.wait()
    wp_a = wsend(0, 0, 224, y, yp)
    wm_b = wsend(1, 0, 224, y, ym)
    wp_b = wsend(1, 0, 224, y, yp)
    wm_a = wsend(0, 0, 224, y, ym)
    locals_[4].wait()
    o_p = send(tok(oa, 0, ROWS), tok(oa, slot(1, 0), ROWS), xp)
    o_m = send(tok(oa, 0, ROWS), tok(oa, slot(2, 0), ROWS), xm)
    o_t = send(tok(oa, 0, ROWS), tok(oa, slot(0, 1), ROWS), twin)

    z_in = []

    def zsend(i, col, dev):
        z_in.append(wsend(i, 0, 224, col, dev))

    wp_a.wait_recv()
    fp_a = wsend(0, 0, 224, y + 3, yp)
    zsend(0, y + 3, zp)
    wm_b.wait_recv()
    fm_b = wsend(1, 0, 224, y + 1, ym)
    zsend(1, y + 1, zm)
    wp_c = wsend(2, 0, 160, y, yp)
    wm_c = wsend(2, 0, 160, y, ym)

    x_p.wait_recv()
    xf_p = send(tok(xa, slot(1, 0), 48), tok(xa, slot(3, 0), 48), xp)
    x_m.wait_recv()
    xf_m = send(tok(xa, slot(2, 0) + 48, 48), tok(xa, slot(3, 0) + 48, 48), xm)
    xt1 = send(tok(xa, slot(1, 0), ROWS), tok(xa, slot(1, 1), ROWS), twin)
    xt2 = send(tok(xa, slot(2, 0), ROWS), tok(xa, slot(2, 1), ROWS), twin)

    wp_b.wait_recv()
    zsend(1, y + 3, zm)
    wm_a.wait_recv()
    zsend(0, y + 1, zp)
    fp_a.wait_recv()
    zsend(0, y + 2, zp)
    fm_b.wait_recv()
    zsend(1, y + 2, zm)

    wp_c.wait_recv()
    fp_c = wsend(2, 0, 80, y + 3, yp)
    wm_c.wait_recv()
    fm_c = wsend(2, 80, 80, y + 1, ym)

    o_p.wait_recv()
    of_p = send(tok(oa, slot(1, 0), 48), tok(oa, slot(3, 0), 48), xp)
    o_m.wait_recv()
    of_m = send(tok(oa, slot(2, 0) + 48, 48), tok(oa, slot(3, 0) + 48, 48), xm)
    ot1 = send(tok(oa, slot(1, 0), ROWS), tok(oa, slot(1, 1), ROWS), twin)
    ot2 = send(tok(oa, slot(2, 0), ROWS), tok(oa, slot(2, 1), ROWS), twin)

    xf_p.wait_recv()
    xt3 = send(tok(xa, slot(3, 0), 48), tok(xa, slot(3, 1), 48), twin)
    xf_m.wait_recv()
    xt4 = send(tok(xa, slot(3, 0) + 48, 48), tok(xa, slot(3, 1) + 48, 48), twin)
    for c in (fp_c, fm_c):
        c.wait_recv()
    for c in z_in:
        c.wait_recv()
    for c in (x_t, o_t, xt1, xt2, ot1, ot2):
        c.wait_recv()

    def project(c0, n, parts=(0, 1, 2)):
        cols = pl.ds(c0, n)
        for part in parts:
            source = oa if part == 2 else xa
            for m in (0, 1):
                rows = pl.ds(HID * part + HID // 2 * m, HID // 2)
                fwd[rows, cols] = nt(w[rows, :], source[cols, :])

    def elementwise(c0, n):
        cols = pl.ds(c0, n)
        for m in range(11):
            a = 32 * m
            g = fwd[a:a + 32, cols].astype(BF16).astype(F32)
            u = fwd[HID + a:HID + a + 32, cols].astype(BF16).astype(F32)
            gh = fwd[2 * HID + a:2 * HID + a + 32, cols].astype(BF16).astype(F32)
            sig = 1.0 / (1.0 + jnp.exp(-g))
            act = g * sig
            l[a:a + 32, cols] = (gh * u * sig * (1.0 + g * (1.0 - sig))).astype(BF16)
            l[HID + a:HID + a + 32, cols] = (gh * act).astype(BF16)
            l[2 * HID + a:2 * HID + a + 32, cols] = (act * u).astype(BF16)

    def shard_cols(r):
        return pl.ds(aligned(lax.rem(y + r, 4) * SHARD, SHARD), SHARD)

    def early(row, n, source):
        pa[row:row + n, :] = nn(l[row:row + n, 0:EARLY], source[0:EARLY, shard_cols(2)])

    def late(row, n, source):
        more = nn(l[row:row + n, EARLY:TOK], source[EARLY:TOK, shard_cols(2)])
        p[AT[2], row:row + n, :] = (pa[row:row + n, :] + more).astype(BF16)

    def whole(r, row, n, source):
        p[AT[r], row:row + n, :] = nn(l[row:row + n, :], source[:, shard_cols(r)]).astype(BF16)

    def early_second(r):
        pz[r, 0:704 - R1, :] = nn(l[R1:704, 0:EARLY], xa[0:EARLY, shard_cols(r)])
        pz[r, 704 - R1:R2, :] = nn(l[704:RP, 0:EARLY], oa[0:EARLY, shard_cols(r)])

    def first_part(r):
        whole(r, 0, R1 // 2, xa)
        whole(r, R1 // 2, R1 // 2, xa)

    def second_part(r):
        more = nn(l[R1:704, EARLY:TOK], xa[EARLY:TOK, shard_cols(r)])
        p[AT[r], R1:704, :] = (pz[r, 0:704 - R1, :] + more).astype(BF16)
        more = nn(l[704:RP, EARLY:TOK], oa[EARLY:TOK, shard_cols(r)])
        p[AT[r], 704:RP, :] = (pz[r, 704 - R1:R2, :] + more).astype(BF16)

    project(0, 256)
    elementwise(0, 256)
    of_p.wait_recv()
    ot3 = send(tok(oa, slot(3, 0), 48), tok(oa, slot(3, 1), 48), twin)
    of_m.wait_recv()
    ot4 = send(tok(oa, slot(3, 0) + 48, 48), tok(oa, slot(3, 1) + 48, 48), twin)
    project(256, EARLY - 256)
    elementwise(256, EARLY - 256)
    xt3.wait_recv()
    xt4.wait_recv()
    project(EARLY, TOK - EARLY, (0, 1))
    early(0, R1 // 2, xa)
    early(R1 // 2, R1 // 2, xa)
    for r in (2, 1, 3, 0):
        early_second(r)
    ot3.wait_recv()
    ot4.wait_recv()
    project(EARLY, TOK - EARLY, (2,))
    elementwise(EARLY, TOK - EARLY)

    class Ring:
        def __init__(self, block, load, b0, b1, c0, c1, plus, minus):
            self.block, self.load = block, load
            self.b0, self.b1, self.c0, self.c1 = b0, b1, c0, c1
            self.plus, self.minus = plus, minus

        def far(self):
            self.far_half(0)
            self.far_half(1)

        def far_half(self, h):
            if h:
                self.a1 = send(self.block(2, 1), self.b1.at[0], self.minus)
            else:
                self.a0 = send(self.block(2, 0), self.b0.at[0], self.plus)

        def near(self):
            self.near_half(1)
            self.near_half(0)

        def near_half(self, h):
            if h:
                self.n1 = send(self.block(1, 1), self.b1.at[1], self.plus)
            else:
                self.n0 = send(self.block(3, 0), self.b0.at[1], self.minus)

        def middle(self):
            self.a0.wait_recv()
            self.c0[...] = (self.b0[0].astype(F32) + self.load(1, 0).astype(F32)).astype(BF16)
            self.e0 = send(self.c0, self.b0.at[2], self.plus)
            self.a1.wait_recv()
            self.c1[...] = (self.b1[0].astype(F32) + self.load(3, 1).astype(F32)).astype(BF16)
            self.e1 = send(self.c1, self.b1.at[2], self.minus)

        def end(self, h):
            for c in ((self.n1, self.e1) if h else (self.n0, self.e0)):
                c.wait_recv()
            got = self.b1 if h else self.b0
            return (self.load(0, h).astype(F32) + got[1].astype(F32) + got[2].astype(F32)).astype(BF16)

    class Spread:
        def __init__(self, base, size, cut):
            self.base, self.size, self.cut = base, size, cut

        def rows(self, r, off, n):
            return out.at[pl.ds(aligned(self.base + self.size * lax.rem(z + r, 4) + off, 16), n)]

        def part(self, r, h):
            return self.rows(r, self.cut * h, self.size - self.cut if h else self.cut)

        def start(self, h):
            ref = self.part(0, h)
            if h:
                self.m1 = send(ref, ref, zm)
                self.p1 = send(ref, ref, zp)
            else:
                self.p0 = send(ref, ref, zp)
                self.m0 = send(ref, ref, zm)

        def middle(self):
            self.p0.wait_recv()
            ref = self.part(3, 0)
            self.f0 = send(ref, ref, zp)
            self.m1.wait_recv()
            ref = self.part(1, 1)
            self.f1 = send(ref, ref, zm)

        def end(self):
            for c in (self.m0, self.p1, self.f0, self.f1):
                c.wait_recv()

    def y_ring(k):
        def rows(h):
            return pl.ds(R1 // 2 * h + PIECE * k, PIECE)
        return Ring(lambda r, h: p.at[AT[r], rows(h)], lambda r, h: p[AT[r], rows(h), :],
                    ya.at[k, 0], ya.at[k, 1], ys.at[k, 0], ys.at[k, 1], yp, ym)

    y_first = [y_ring(0), y_ring(1)]

    pair_a = (z + 1 - 2 * half, y, t)
    pair_b = (lax.rem(z + 3 + 2 * half, 4), y, t)

    class Exchange:
        def __init__(self, i):
            self.i, self.rows = i, pl.ds(PIECE * i, PIECE)
            self.first, self.second = (pair_a, pair_b) if i < 2 else (pair_b, pair_a)

        def start(self):
            self.c0 = send(yr.at[self.rows], got.at[0, self.rows], self.first)

        def middle(self):
            self.c0.wait_recv()
            half_sum[self.rows, :] = (yr[self.rows, :].astype(F32) + got[0, self.rows, :].astype(F32)).astype(BF16)
            self.c1 = send(half_sum.at[self.rows], got.at[1, self.rows], self.second)

        def end(self):
            self.c1.wait_recv()
            out[self.rows, :] = (half_sum[self.rows, :].astype(F32) + got[1, self.rows, :].astype(F32)).astype(BF16)

    swaps = [Exchange(i) for i in range(4)]

    def q2(r, h):
        return pl.ds(aligned(R1 + Q2 * lax.rem(z + r, 4) + H0 * h, 16), H1 if h else H0)

    def z_ring(k):
        two = pl.ds(2 * k, 2)
        return Ring(lambda r, h: p.at[two, q2(r, h)], lambda r, h: p[two, q2(r, h), :],
                    zb0.at[k], zb1.at[k], zc0.at[k], zc1.at[k], zp, zm)

    z_first = [z_ring(0), z_ring(1)]

    def zh(h):
        return pl.ds(H0 * h, H1 if h else H0)
    z_then = Ring(lambda r, h: zr.at[AT[r], zh(h)], lambda r, h: zr[AT[r], zh(h), :],
                  yb0, yb1, yc0, yc1, yp, ym)
    z_out = Spread(R1, Q2, H0)

    for h in (0, 1):
        late(R1 // 2 * h, R1 // 2, xa)
        y_first[0].far_half(h)
        y_first[1].far_half(h)
    for r in (2, 1, 3, 0):
        second_part(r)
    z_first[0].far()
    z_first[1].far()
    z_first[0].near()
    z_first[1].near()
    first_part(1)
    first_part(3)
    y_first[0].near()
    y_first[1].near()

    lt[...] = l[0:704, :].T

    def token_grads(rel):
        rows = jnp.concatenate([lt[slot(k, rel):slot(k, rel) + ROWS, :] for k in range(4)], axis=0)
        return nn(rows, w[0:704, :])

    pb[...] = token_grads(1).astype(BF16)
    pair = send(pb, rb, twin)
    s0[...] = token_grads(0)

    y_first[0].middle()
    z_first[0].middle()
    y_first[1].middle()
    z_first[1].middle()
    pair.wait_recv()
    sb[...] = (s0[...] + rb[...].astype(F32)).astype(BF16)
    chip = {0: 0, 3: 1, 1: 2, 2: 3}
    def xh(r, h):
        return pl.ds(ROWS * chip[r] + 48 * h, 48)
    x_ring = Ring(lambda r, h: sb.at[xh(r, h)], lambda r, h: sb[xh(r, h), :],
                  xr.at[0], xr.at[1], xs.at[0], xs.at[1], xp, xm)
    x_ring.far()
    x_ring.near()
    first_part(0)
    drain(16)

    for h in (0, 1):
        zr[0:2, zh(h), :] = z_first[0].end(h)
    z_then.far()
    z_then.near_half(1)
    for k in (0, 1):
        for h in (0, 1):
            yr[pl.ds(R1 // 2 * h + PIECE * k, PIECE), :] = y_first[k].end(h)
            swaps[2 * h + k].start()
        if k == 0:
            for h in (0, 1):
                zr[2:4, zh(h), :] = z_first[1].end(h)
            z_then.near_half(0)
    drain(20)
    x_ring.middle()
    z_then.middle()
    for h in (0, 1):
        out[z_out_rows(z, h), :] = z_then.end(h)
        z_out.start(h)
    for i in (0, 2, 1, 3):
        swaps[i].middle()
    drain(8)
    gi_ref[0:48, :] = x_ring.end(0)
    gi_ref[48:96, :] = x_ring.end(1)
    z_out.middle()
    for i in (0, 2, 1, 3):
        swaps[i].end()
    z_out.end()
    drain()


def z_out_rows(z, h):
    return pl.ds(pl.multiple_of(R1 + Q2 * z + H0 * h, 16), H1 if h else H0)


def finish(factor, gi_ref, dw_ref, gi_hbm, og_hbm, ou_hbm, od_hbm, gi, og, ou, od, sems):
    copies = []
    for i, (buf, dst) in enumerate(((gi, gi_hbm), (og, og_hbm), (ou, ou_hbm), (od, od_hbm))):
        if i == 0:
            buf[...] = gi_ref[...]
        else:
            buf[...] = dw_ref[HID * (i - 1):HID * i, :].astype(F32) * factor
        copies.append(pltpu.make_async_copy(buf, dst, sems.at[i]))
        copies[-1].start()
    for c in copies:
        c.wait()


def body(tokens_in, out_grad, gate_weight, up_weight, down_weight):
    factor = (ROWS * 128) ** (-0.5)
    vmem = pl.BlockSpec(memory_space=pltpu.VMEM)
    hbm = pl.BlockSpec(memory_space=pl.ANY)
    grad_in, sums = pl.pallas_call(
        kernel,
        name="ffn_backward",
        out_shape=(pltpu.VMEM((ROWS, WIDTH), BF16), pltpu.VMEM((RP, SHARD), BF16)),
        in_specs=[pl.BlockSpec(memory_space=pl.ANY)] * 5,
        out_specs=(vmem, vmem),
        scratch_shapes=[
            pltpu.VMEM((TOK, WIDTH), BF16),
            pltpu.VMEM((TOK, WIDTH), BF16),
            pltpu.VMEM((3 * HID, WIDTH), BF16),
            pltpu.VMEM((3 * HID, TOK), F32),
            pltpu.VMEM((RP, TOK), BF16),
            pltpu.VMEM((TOK, 2 * HID), BF16),
            pltpu.VMEM((R1, SHARD), F32),
            pltpu.VMEM((4, R2, SHARD), F32),
            pltpu.VMEM((4, RP, SHARD), BF16),
            pltpu.VMEM((384, WIDTH), BF16),
            pltpu.VMEM((384, WIDTH), BF16),
            pltpu.VMEM((384, WIDTH), F32),
            pltpu.VMEM((384, WIDTH), BF16),
            pltpu.VMEM((2, 3, 48, WIDTH), BF16),
            pltpu.VMEM((2, 48, WIDTH), BF16),
            pltpu.VMEM((2, 2, 3, PIECE, SHARD), BF16),
            pltpu.VMEM((2, 2, PIECE, SHARD), BF16),
            pltpu.VMEM((R1, SHARD), BF16),
            pltpu.VMEM((2, R1, SHARD), BF16),
            pltpu.VMEM((R1, SHARD), BF16),
            pltpu.VMEM((2, 3, 2, H0, SHARD), BF16),
            pltpu.VMEM((2, 3, 2, H1, SHARD), BF16),
            pltpu.VMEM((2, 2, H0, SHARD), BF16),
            pltpu.VMEM((2, 2, H1, SHARD), BF16),
            pltpu.VMEM((4, Q2, SHARD), BF16),
            pltpu.VMEM((3, H0, SHARD), BF16),
            pltpu.VMEM((3, H1, SHARD), BF16),
            pltpu.VMEM((H0, SHARD), BF16),
            pltpu.VMEM((H1, SHARD), BF16),
            pltpu.SemaphoreType.DMA((5,)),
            pltpu.SemaphoreType.DMA((112,)),
            pltpu.SemaphoreType.DMA((112,)),
        ],
        compiler_params=pltpu.CompilerParams(collective_id=0, has_side_effects=True),
    )(tokens_in, out_grad, gate_weight.T, up_weight.T, down_weight)
    grad_in, gg, gu, gd = pl.pallas_call(
        functools.partial(finish, factor),
        name="finish",
        out_shape=(jax.ShapeDtypeStruct((ROWS, WIDTH), BF16),) + (jax.ShapeDtypeStruct((HID, SHARD), F32),) * 3,
        in_specs=[vmem, vmem],
        out_specs=(hbm,) * 4,
        scratch_shapes=[pltpu.VMEM((ROWS, WIDTH), BF16)] + [pltpu.VMEM((HID, SHARD), F32)] * 3
        + [pltpu.SemaphoreType.DMA((4,))],
        compiler_params=pltpu.CompilerParams(vmem_limit_bytes=8 << 20),
    )(grad_in, sums)
    return grad_in, gg.T, gu.T, gd


def solution(mesh):
    return jax.shard_map(
        body,
        mesh=mesh,
        in_specs=(
            P(("rep", "fs", "tp"), None),
            P(("rep", "fs", "tp"), None),
            P("fs", "tp"),
            P("fs", "tp"),
            P("tp", "fs"),
        ),
        out_specs=(P(("rep", "fs", "tp"), None), P("fs", "tp"), P("fs", "tp"), P("tp", "fs")),
        check_vma=False,
    )
```

```python
import functools

import jax
import jax.numpy as jnp
from jax import lax
from jax.experimental import pallas as pl
from jax.experimental.pallas import tpu as pltpu
from jax.sharding import PartitionSpec as P

MESH = pl.DeviceIdType.MESH
F32 = jnp.float32
BF16 = jnp.bfloat16

ROWS = 96
WIDTH = 1024
HID = 352
SHARD = 256
TOK = 768
EARLY = 512
R1 = 576
R2 = 512
RP = R1 + R2
PIECE, Q2 = R1 // 4, R2 // 4
H0, H1 = 64, 64


AT = (3, 0, 1, 2)


def nt(a, b):
    return lax.dot_general(a, b, (((1,), (1,)), ((), ())), preferred_element_type=F32)


def nn(a, b):
    return lax.dot_general(a, b, (((1,), (0,)), ((), ())), preferred_element_type=F32)


def aligned(value, by):
    return pl.multiple_of(value, by)


def kernel(x_hbm, o_hbm, g_hbm, u_hbm, d_hbm, gi_ref, out,
           xa, oa, w, fwd, l, lt, pa, pz, p, pb, rb, s0, sb, xr, xs,
           ya, ys, yr, got, half_sum, zb0, zb1, zc0, zc1, zr, yb0, yb1, yc0, yc1,
           ls, ss, rs):
    z = lax.axis_index("rep")
    y = lax.axis_index("fs")
    t = lax.axis_index("tp")
    core = lax.rem(t, 2)
    half = lax.rem(z, 2)
    xp = (z, y, lax.rem(t + 2, 8))
    xm = (z, y, lax.rem(t + 6, 8))
    twin = (z, y, t + 1 - 2 * core)
    yp = (z, lax.rem(y + 1, 4), t)
    ym = (z, lax.rem(y + 3, 4), t)
    zp = (lax.rem(z + 1, 4), y, t)
    zm = (lax.rem(z + 3, 4), y, t)

    counter = [0]
    started = []

    def send(src, dst, dev):
        i = counter[0]
        counter[0] += 1
        copy = pltpu.make_async_remote_copy(
            src_ref=src, dst_ref=dst, send_sem=ss.at[i], recv_sem=rs.at[i],
            device_id=dev, device_id_type=MESH)
        copy.start()
        started.append(copy)
        return copy

    def drain(keep=0):
        while len(started) > keep:
            started.pop(0).wait_send()

    mine = pl.ds(aligned(y * SHARD, SHARD), SHARD)
    locals_ = [
        pltpu.make_async_copy(x_hbm, xa.at[pl.ds(0, ROWS)], ls.at[0]),
        pltpu.make_async_copy(g_hbm, w.at[pl.ds(0, HID), mine], ls.at[1]),
        pltpu.make_async_copy(u_hbm, w.at[pl.ds(HID, HID), mine], ls.at[2]),
        pltpu.make_async_copy(d_hbm, w.at[pl.ds(2 * HID, HID), mine], ls.at[3]),
        pltpu.make_async_copy(o_hbm, oa.at[pl.ds(0, ROWS)], ls.at[4]),
    ]
    for c in locals_:
        c.start()

    barrier = pltpu.get_barrier_semaphore()
    for dev in (xp, xm, twin, yp, ym, zp, zm):
        pl.semaphore_signal(barrier, inc=1, device_id=dev, device_id_type=MESH)
    l[pl.ds(3 * HID, RP - 3 * HID), :] = jnp.zeros((RP - 3 * HID, TOK), BF16)
    pl.semaphore_wait(barrier, 7)

    def slot(k, rel):
        return 2 * ROWS * k + ROWS * rel

    def tok(ref, row, n):
        return ref.at[pl.ds(row, n)]

    my_rows = [aligned(608 * half, 16), aligned(608 * half + 224, 16), 448]

    def wblk(row, n, col):
        return w.at[pl.ds(row, n), pl.ds(aligned(lax.rem(col, 4) * SHARD, SHARD), SHARD)]

    def wsend(i, off, n, col, dev):
        ref = wblk(my_rows[i] + off if off else my_rows[i], n, col)
        return send(ref, ref, dev)

    for c in locals_[:1]:
        c.wait()
    x_p = send(tok(xa, 0, ROWS), tok(xa, slot(1, 0), ROWS), xp)
    x_m = send(tok(xa, 0, ROWS), tok(xa, slot(2, 0), ROWS), xm)
    x_t = send(tok(xa, 0, ROWS), tok(xa, slot(0, 1), ROWS), twin)
    for c in locals_[1:4]:
        c.wait()
    wp_a = wsend(0, 0, 224, y, yp)
    wm_b = wsend(1, 0, 224, y, ym)
    wp_b = wsend(1, 0, 224, y, yp)
    wm_a = wsend(0, 0, 224, y, ym)
    locals_[4].wait()
    o_p = send(tok(oa, 0, ROWS), tok(oa, slot(1, 0), ROWS), xp)
    o_m = send(tok(oa, 0, ROWS), tok(oa, slot(2, 0), ROWS), xm)
    o_t = send(tok(oa, 0, ROWS), tok(oa, slot(0, 1), ROWS), twin)

    z_in = []

    def zsend(i, col, dev):
        z_in.append(wsend(i, 0, 224, col, dev))

    wp_a.wait_recv()
    fp_a = wsend(0, 0, 224, y + 3, yp)
    zsend(0, y + 3, zp)
    wm_b.wait_recv()
    fm_b = wsend(1, 0, 224, y + 1, ym)
    zsend(1, y + 1, zm)
    wp_c = wsend(2, 0, 160, y, yp)
    wm_c = wsend(2, 0, 160, y, ym)

    x_p.wait_recv()
    xf_p = send(tok(xa, slot(1, 0), 48), tok(xa, slot(3, 0), 48), xp)
    x_m.wait_recv()
    xf_m = send(tok(xa, slot(2, 0) + 48, 48), tok(xa, slot(3, 0) + 48, 48), xm)
    xt1 = send(tok(xa, slot(1, 0), ROWS), tok(xa, slot(1, 1), ROWS), twin)
    xt2 = send(tok(xa, slot(2, 0), ROWS), tok(xa, slot(2, 1), ROWS), twin)

    wp_b.wait_recv()
    zsend(1, y + 3, zm)
    wm_a.wait_recv()
    zsend(0, y + 1, zp)
    fp_a.wait_recv()
    zsend(0, y + 2, zp)
    fm_b.wait_recv()
    zsend(1, y + 2, zm)

    wp_c.wait_recv()
    fp_c = wsend(2, 0, 80, y + 3, yp)
    wm_c.wait_recv()
    fm_c = wsend(2, 80, 80, y + 1, ym)

    o_p.wait_recv()
    of_p = send(tok(oa, slot(1, 0), 48), tok(oa, slot(3, 0), 48), xp)
    o_m.wait_recv()
    of_m = send(tok(oa, slot(2, 0) + 48, 48), tok(oa, slot(3, 0) + 48, 48), xm)
    ot1 = send(tok(oa, slot(1, 0), ROWS), tok(oa, slot(1, 1), ROWS), twin)
    ot2 = send(tok(oa, slot(2, 0), ROWS), tok(oa, slot(2, 1), ROWS), twin)

    xf_p.wait_recv()
    xt3 = send(tok(xa, slot(3, 0), 48), tok(xa, slot(3, 1), 48), twin)
    xf_m.wait_recv()
    xt4 = send(tok(xa, slot(3, 0) + 48, 48), tok(xa, slot(3, 1) + 48, 48), twin)
    for c in (fp_c, fm_c):
        c.wait_recv()
    for c in z_in:
        c.wait_recv()
    for c in (x_t, o_t, xt1, xt2, ot1, ot2):
        c.wait_recv()

    def project(c0, n, parts=(0, 1, 2)):
        cols = pl.ds(c0, n)
        for part in parts:
            source = oa if part == 2 else xa
            for m in (0, 1):
                rows = pl.ds(HID * part + HID // 2 * m, HID // 2)
                fwd[rows, cols] = nt(w[rows, :], source[cols, :])

    def elementwise(c0, n):
        cols = pl.ds(c0, n)
        for m in range(11):
            a = 32 * m
            g = fwd[a:a + 32, cols].astype(BF16).astype(F32)
            u = fwd[HID + a:HID + a + 32, cols].astype(BF16).astype(F32)
            gh = fwd[2 * HID + a:2 * HID + a + 32, cols].astype(BF16).astype(F32)
            sig = jax.nn.sigmoid(g)
            act = g * sig
            l[a:a + 32, cols] = (gh * u * sig * (1.0 + g * (1.0 - sig))).astype(BF16)
            l[HID + a:HID + a + 32, cols] = (gh * act).astype(BF16)
            l[2 * HID + a:2 * HID + a + 32, cols] = (act * u).astype(BF16)

    def shard_cols(r):
        return pl.ds(aligned(lax.rem(y + r, 4) * SHARD, SHARD), SHARD)

    def early(row, n, source):
        pa[row:row + n, :] = nn(l[row:row + n, 0:EARLY], source[0:EARLY, shard_cols(2)])

    def late(row, n, source):
        more = nn(l[row:row + n, EARLY:TOK], source[EARLY:TOK, shard_cols(2)])
        p[AT[2], row:row + n, :] = (pa[row:row + n, :] + more).astype(BF16)

    def whole(r, row, n, source):
        p[AT[r], row:row + n, :] = nn(l[row:row + n, :], source[:, shard_cols(r)]).astype(BF16)

    def early_second(r):
        pz[r, 0:704 - R1, :] = nn(l[R1:704, 0:EARLY], xa[0:EARLY, shard_cols(r)])
        pz[r, 704 - R1:R2, :] = nn(l[704:RP, 0:EARLY], oa[0:EARLY, shard_cols(r)])

    def first_part(r):
        whole(r, 0, R1 // 2, xa)
        whole(r, R1 // 2, R1 // 2, xa)

    def second_part(r):
        more = nn(l[R1:704, EARLY:TOK], xa[EARLY:TOK, shard_cols(r)])
        p[AT[r], R1:704, :] = (pz[r, 0:704 - R1, :] + more).astype(BF16)
        more = nn(l[704:RP, EARLY:TOK], oa[EARLY:TOK, shard_cols(r)])
        p[AT[r], 704:RP, :] = (pz[r, 704 - R1:R2, :] + more).astype(BF16)

    project(0, 256)
    elementwise(0, 256)
    of_p.wait_recv()
    ot3 = send(tok(oa, slot(3, 0), 48), tok(oa, slot(3, 1), 48), twin)
    of_m.wait_recv()
    ot4 = send(tok(oa, slot(3, 0) + 48, 48), tok(oa, slot(3, 1) + 48, 48), twin)
    project(256, EARLY - 256)
    elementwise(256, EARLY - 256)
    xt3.wait_recv()
    xt4.wait_recv()
    project(EARLY, TOK - EARLY, (0, 1))
    early(0, R1 // 2, xa)
    early(R1 // 2, R1 // 2, xa)
    for r in (2, 1, 3, 0):
        early_second(r)
    ot3.wait_recv()
    ot4.wait_recv()
    project(EARLY, TOK - EARLY, (2,))
    elementwise(EARLY, TOK - EARLY)

    class Ring:
        def __init__(self, block, load, b0, b1, c0, c1, plus, minus):
            self.block, self.load = block, load
            self.b0, self.b1, self.c0, self.c1 = b0, b1, c0, c1
            self.plus, self.minus = plus, minus

        def far(self):
            self.far_half(0)
            self.far_half(1)

        def far_half(self, h):
            if h:
                self.a1 = send(self.block(2, 1), self.b1.at[0], self.minus)
            else:
                self.a0 = send(self.block(2, 0), self.b0.at[0], self.plus)

        def near(self):
            self.near_half(1)
            self.near_half(0)

        def near_half(self, h):
            if h:
                self.n1 = send(self.block(1, 1), self.b1.at[1], self.plus)
            else:
                self.n0 = send(self.block(3, 0), self.b0.at[1], self.minus)

        def middle(self):
            self.a0.wait_recv()
            self.c0[...] = (self.b0[0].astype(F32) + self.load(1, 0).astype(F32)).astype(BF16)
            self.e0 = send(self.c0, self.b0.at[2], self.plus)
            self.a1.wait_recv()
            self.c1[...] = (self.b1[0].astype(F32) + self.load(3, 1).astype(F32)).astype(BF16)
            self.e1 = send(self.c1, self.b1.at[2], self.minus)

        def end(self, h):
            for c in ((self.n1, self.e1) if h else (self.n0, self.e0)):
                c.wait_recv()
            got = self.b1 if h else self.b0
            return (self.load(0, h).astype(F32) + got[1].astype(F32) + got[2].astype(F32)).astype(BF16)

    class Spread:
        def __init__(self, base, size, cut):
            self.base, self.size, self.cut = base, size, cut

        def rows(self, r, off, n):
            return out.at[pl.ds(aligned(self.base + self.size * lax.rem(z + r, 4) + off, 16), n)]

        def part(self, r, h):
            return self.rows(r, self.cut * h, self.size - self.cut if h else self.cut)

        def start(self, h):
            ref = self.part(0, h)
            if h:
                self.m1 = send(ref, ref, zm)
                self.p1 = send(ref, ref, zp)
            else:
                self.p0 = send(ref, ref, zp)
                self.m0 = send(ref, ref, zm)

        def middle(self):
            self.p0.wait_recv()
            ref = self.part(3, 0)
            self.f0 = send(ref, ref, zp)
            self.m1.wait_recv()
            ref = self.part(1, 1)
            self.f1 = send(ref, ref, zm)

        def end(self):
            for c in (self.m0, self.p1, self.f0, self.f1):
                c.wait_recv()

    def y_ring(k):
        def rows(h):
            return pl.ds(R1 // 2 * h + PIECE * k, PIECE)
        return Ring(lambda r, h: p.at[AT[r], rows(h)], lambda r, h: p[AT[r], rows(h), :],
                    ya.at[k, 0], ya.at[k, 1], ys.at[k, 0], ys.at[k, 1], yp, ym)

    y_first = [y_ring(0), y_ring(1)]

    pair_a = (z + 1 - 2 * half, y, t)
    pair_b = (lax.rem(z + 3 + 2 * half, 4), y, t)

    class Exchange:
        def __init__(self, i):
            self.i, self.rows = i, pl.ds(PIECE * i, PIECE)
            self.first, self.second = (pair_a, pair_b) if i < 2 else (pair_b, pair_a)

        def start(self):
            self.c0 = send(yr.at[self.rows], got.at[0, self.rows], self.first)

        def middle(self):
            self.c0.wait_recv()
            half_sum[self.rows, :] = (yr[self.rows, :].astype(F32) + got[0, self.rows, :].astype(F32)).astype(BF16)
            self.c1 = send(half_sum.at[self.rows], got.at[1, self.rows], self.second)

        def end(self):
            self.c1.wait_recv()
            out[self.rows, :] = (half_sum[self.rows, :].astype(F32) + got[1, self.rows, :].astype(F32)).astype(BF16)

    swaps = [Exchange(i) for i in range(4)]

    def q2(r, h):
        return pl.ds(aligned(R1 + Q2 * lax.rem(z + r, 4) + H0 * h, 16), H1 if h else H0)

    def z_ring(k):
        two = pl.ds(2 * k, 2)
        return Ring(lambda r, h: p.at[two, q2(r, h)], lambda r, h: p[two, q2(r, h), :],
                    zb0.at[k], zb1.at[k], zc0.at[k], zc1.at[k], zp, zm)

    z_first = [z_ring(0), z_ring(1)]

    def zh(h):
        return pl.ds(H0 * h, H1 if h else H0)
    z_then = Ring(lambda r, h: zr.at[AT[r], zh(h)], lambda r, h: zr[AT[r], zh(h), :],
                  yb0, yb1, yc0, yc1, yp, ym)
    z_out = Spread(R1, Q2, H0)

    for h in (0, 1):
        late(R1 // 2 * h, R1 // 2, xa)
        y_first[0].far_half(h)
        y_first[1].far_half(h)
    for r in (2, 1, 3, 0):
        second_part(r)
    z_first[0].far()
    z_first[1].far()
    z_first[0].near()
    z_first[1].near()
    first_part(1)
    first_part(3)
    y_first[0].near()
    y_first[1].near()

    lt[...] = l[0:704, :].T

    def token_grads(rel):
        rows = jnp.concatenate([lt[slot(k, rel):slot(k, rel) + ROWS, :] for k in range(4)], axis=0)
        return nn(rows, w[0:704, :])

    pb[...] = token_grads(1).astype(BF16)
    pair = send(pb, rb, twin)
    y_first[0].middle()
    s0[...] = token_grads(0)

    z_first[0].middle()
    y_first[1].middle()
    z_first[1].middle()
    pair.wait_recv()
    sb[...] = (s0[...] + rb[...].astype(F32)).astype(BF16)
    chip = {0: 0, 3: 1, 1: 2, 2: 3}
    def xh(r, h):
        return pl.ds(ROWS * chip[r] + 48 * h, 48)
    x_ring = Ring(lambda r, h: sb.at[xh(r, h)], lambda r, h: sb[xh(r, h), :],
                  xr.at[0], xr.at[1], xs.at[0], xs.at[1], xp, xm)
    x_ring.far()
    x_ring.near()
    first_part(0)
    drain(16)

    for h in (0, 1):
        zr[0:2, zh(h), :] = z_first[0].end(h)
    z_then.far()
    z_then.near_half(1)
    for k in (0, 1):
        for h in (0, 1):
            yr[pl.ds(R1 // 2 * h + PIECE * k, PIECE), :] = y_first[k].end(h)
            swaps[2 * h + k].start()
        if k == 0:
            for h in (0, 1):
                zr[2:4, zh(h), :] = z_first[1].end(h)
            z_then.near_half(0)
    drain(20)
    x_ring.middle()
    z_then.middle()
    for h in (0, 1):
        out[z_out_rows(z, h), :] = z_then.end(h)
        z_out.start(h)
    for i in (0, 2, 1, 3):
        swaps[i].middle()
    drain(8)
    gi_ref[0:48, :] = x_ring.end(0)
    gi_ref[48:96, :] = x_ring.end(1)
    z_out.middle()
    for i in (0, 2, 1, 3):
        swaps[i].end()
    z_out.end()
    drain()


def z_out_rows(z, h):
    return pl.ds(pl.multiple_of(R1 + Q2 * z + H0 * h, 16), H1 if h else H0)


def finish(factor, gi_ref, dw_ref, gi_hbm, og_hbm, ou_hbm, od_hbm, gi, og, ou, od, sems):
    copies = []
    for i, (buf, dst) in enumerate(((gi, gi_hbm), (og, og_hbm), (ou, ou_hbm), (od, od_hbm))):
        if i == 0:
            buf[...] = gi_ref[...]
        else:
            buf[...] = dw_ref[HID * (i - 1):HID * i, :].astype(F32) * factor
        copies.append(pltpu.make_async_copy(buf, dst, sems.at[i]))
        copies[-1].start()
    for c in copies:
        c.wait()


def body(tokens_in, out_grad, gate_weight, up_weight, down_weight):
    factor = (ROWS * 128) ** (-0.5)
    vmem = pl.BlockSpec(memory_space=pltpu.VMEM)
    hbm = pl.BlockSpec(memory_space=pl.ANY)
    grad_in, sums = pl.pallas_call(
        kernel,
        name="ffn_backward",
        out_shape=(pltpu.VMEM((ROWS, WIDTH), BF16), pltpu.VMEM((RP, SHARD), BF16)),
        in_specs=[pl.BlockSpec(memory_space=pl.ANY)] * 5,
        out_specs=(vmem, vmem),
        scratch_shapes=[
            pltpu.VMEM((TOK, WIDTH), BF16),
            pltpu.VMEM((TOK, WIDTH), BF16),
            pltpu.VMEM((3 * HID, WIDTH), BF16),
            pltpu.VMEM((3 * HID, TOK), F32),
            pltpu.VMEM((RP, TOK), BF16),
            pltpu.VMEM((TOK, 2 * HID), BF16),
            pltpu.VMEM((R1, SHARD), F32),
            pltpu.VMEM((4, R2, SHARD), F32),
            pltpu.VMEM((4, RP, SHARD), BF16),
            pltpu.VMEM((384, WIDTH), BF16),
            pltpu.VMEM((384, WIDTH), BF16),
            pltpu.VMEM((384, WIDTH), F32),
            pltpu.VMEM((384, WIDTH), BF16),
            pltpu.VMEM((2, 3, 48, WIDTH), BF16),
            pltpu.VMEM((2, 48, WIDTH), BF16),
            pltpu.VMEM((2, 2, 3, PIECE, SHARD), BF16),
            pltpu.VMEM((2, 2, PIECE, SHARD), BF16),
            pltpu.VMEM((R1, SHARD), BF16),
            pltpu.VMEM((2, R1, SHARD), BF16),
            pltpu.VMEM((R1, SHARD), BF16),
            pltpu.VMEM((2, 3, 2, H0, SHARD), BF16),
            pltpu.VMEM((2, 3, 2, H1, SHARD), BF16),
            pltpu.VMEM((2, 2, H0, SHARD), BF16),
            pltpu.VMEM((2, 2, H1, SHARD), BF16),
            pltpu.VMEM((4, Q2, SHARD), BF16),
            pltpu.VMEM((3, H0, SHARD), BF16),
            pltpu.VMEM((3, H1, SHARD), BF16),
            pltpu.VMEM((H0, SHARD), BF16),
            pltpu.VMEM((H1, SHARD), BF16),
            pltpu.SemaphoreType.DMA((5,)),
            pltpu.SemaphoreType.DMA((112,)),
            pltpu.SemaphoreType.DMA((112,)),
        ],
        compiler_params=pltpu.CompilerParams(collective_id=0, has_side_effects=True),
    )(tokens_in, out_grad, gate_weight.T, up_weight.T, down_weight)
    grad_in, gg, gu, gd = pl.pallas_call(
        functools.partial(finish, factor),
        name="finish",
        out_shape=(jax.ShapeDtypeStruct((ROWS, WIDTH), BF16),) + (jax.ShapeDtypeStruct((HID, SHARD), F32),) * 3,
        in_specs=[vmem, vmem],
        out_specs=(hbm,) * 4,
        scratch_shapes=[pltpu.VMEM((ROWS, WIDTH), BF16)] + [pltpu.VMEM((HID, SHARD), F32)] * 3
        + [pltpu.SemaphoreType.DMA((4,))],
        compiler_params=pltpu.CompilerParams(vmem_limit_bytes=8 << 20),
    )(grad_in, sums)
    return grad_in, gg.T, gu.T, gd


def solution(mesh):
    return jax.shard_map(
        body,
        mesh=mesh,
        in_specs=(
            P(("rep", "fs", "tp"), None),
            P(("rep", "fs", "tp"), None),
            P("fs", "tp"),
            P("fs", "tp"),
            P("tp", "fs"),
        ),
        out_specs=(P(("rep", "fs", "tp"), None), P("fs", "tp"), P("fs", "tp"), P("tp", "fs")),
        check_vma=False,
    )
```
